32 devices in a mesh: ep: 8 (over z, core), tp: 4 (over y, x).
Axes of the slice: x: 2, y: 2, z: 4, core: 2. Of those that a mesh axis runs over, the one named last changes fastest.
Arguments:
- q_latent: bfloat16 [4096, 512], P('ep'), may hold values from -6 to 6
- kv_latent: bfloat16 [4096, 256], P('ep'), may hold values from -6 to 6
- rope_key: bfloat16 [4096, 32], P('ep'), may hold values from -400 to 400
- q_gain: bfloat16 [512], replicated, may hold values from 0.099609375 to 1.8984375
- kv_gain: bfloat16 [256], replicated, may hold values from 0.099609375 to 1.8984375
- w_q_nope: bfloat16 [512, 1024], P(None, 'tp'), may hold values from -0.25 to 0.25
- w_q_rope: bfloat16 [512, 512], P(None, 'tp'), may hold values from -0.25 to 0.25
- w_k_nope: bfloat16 [256, 1024], P(None, 'tp'), may hold values from -0.375 to 0.375
- w_value: bfloat16 [256, 1024], P(None, 'tp'), may hold values from -0.375 to 0.375
- w_out: bfloat16 [1024, 2048], P('tp'), may hold values from -5.375 to 5.375
- tokens_b: bfloat16 [1024, 2048], P('ep'), may hold values from -6 to 6
- norm_gain_b: bfloat16 [2048], replicated, may hold values from 0.099609375 to 1.8984375
- routes: int32 [1024, 2], P('ep'), may hold values from 0 to 7, all different within a row; in each aligned block of 128 rows (0 to 127, 128 to 255, ...) at most 48 rows name the same one
- route_logits: float32 [1024, 2], P('ep'), may hold values from -6 to 6
- w_gate: bfloat16 [8, 2048, 4096], P('ep', None, 'tp'), may hold values from -0.125 to 0.125
- w_up: bfloat16 [8, 2048, 4096], P('ep', None, 'tp'), may hold values from -0.125 to 0.125
- w_down: bfloat16 [8, 4096, 2048], P('ep', 'tp'), may hold values from -0.125 to 0.125
Outputs:
- mixer_out: bfloat16 [4096, 2048], P(('ep', 'tp'))
- expert_mix: bfloat16 [1024, 2048], P('ep', 'tp')
The draws below stay inside these ranges and needn't reach their ends.
Inputs may be any that keep to these rules, and one draw needn't show every extreme that they name: `routes`: each row names two different experts. In each aligned block of 128 rows (the rows of one index of ep) no expert is named by more than 48 rows, and in every draw some expert is named by exactly 48 rows of some block.
All inputs are finite; a program needn't handle non-finite values.
Results may differ from the reference program's by a relative error of at most 0.022.
The reference program's roundings to bfloat16 on the way count: a program that leaves them out, or rounds other values in their place, can miss the bound.
Values may be sent and summed in bfloat16 or wider, within the bound.
A program may use at most 128 MiB of HBM per device.

```python
import math
import jax
import jax.numpy as jnp
import numpy as np
from jax import lax

D = 2048
HEADS = 16
NOPE = 64
ROPE = 32
VDIM = 64
QLAT = 512
KVLAT = 256
FFE = 4096
R_B = 128
TOK_A = 4096
TOK_B = 1024
EXPERTS = 8
CAP = 48
N_EP = 8
N_TP = 4


def draw_rope_key(key, part):
    base = jax.random.normal(jax.random.fold_in(key, 11), (TOK_A, ROPE), jnp.float32)
    return jnp.clip(base, -400.0, 400.0).astype(jnp.bfloat16)


def with_spikes(drawn, stream_key, source, target, blocks, factor):
    owner, partner = [(jnp.arange(drawn.shape[axis_at]) // (drawn.shape[axis_at] // blocks)).reshape([-1 if axis == axis_at else 1 for axis in range(drawn.ndim)]) for axis_at in (source, target)]
    chosen = jax.random.permutation(stream_key, blocks)[partner]
    strong = (owner == chosen) | (owner == (partner + blocks // 2) % blocks)
    return jnp.where(strong, factor * drawn, drawn)


def level_of(own_key, extent, cuts, low, top_value):
    level = 1.0
    for axis_at, blocks in cuts:
        steps = jax.random.uniform(jax.random.fold_in(jax.random.fold_in(own_key, 6), axis_at), (blocks,), jnp.float32, low / len(cuts), top_value / len(cuts))
        level = level * jnp.repeat(jnp.exp(steps), extent[axis_at] // blocks).reshape((-1,) + (1,) * (len(extent) - 1 - axis_at))
    return level


def assign_block(stream_key, own, number, rows, number_of, top, most, slope):
    ranking = jax.random.permutation(stream_key, number_of)
    crowded, usual = load_shares(number_of, rows * top, most, slope, True), load_shares(number_of, rows * top, most, slope, False)
    places = jnp.arange(number_of)

    def named(sizes, turn):
        used = int((sizes > 0).sum())
        fixed = max(1, used // 4)
        passed = fixed + (places - fixed + turn * (used - fixed)) % max(1, number_of - fixed)
        return jnp.zeros((number_of,), jnp.int32).at[ranking[jnp.where(places < fixed, places, passed)]].set(jnp.asarray(sizes, jnp.int32))

    sizes = jnp.where(number % 4 == 0, named(crowded, number // 4), named(usual, number - number // 4 - 1))
    mixed = jax.random.permutation(jax.random.fold_in(own, 3), number_of)
    donor, sink = mixed[0:number_of // 2 * 2:2], mixed[1:number_of // 2 * 2:2]
    margin = jnp.minimum(sizes[donor] - 1, most - sizes[sink]) // 2
    margin = jnp.where((donor == ranking[0]) | (sink == ranking[0]) | (sizes[sink] == 0), 0, jnp.maximum(margin, 0))
    passed = jax.random.randint(jax.random.fold_in(own, 4), (number_of // 2,), 0, 1 << 20) % (margin + 1)
    sizes = sizes.at[donor].add(-passed).at[sink].add(passed)
    items = jnp.searchsorted(jnp.cumsum(sizes), jnp.arange(rows * top), side="right").astype(jnp.int32)
    grid = items.reshape(top, rows).T
    grid = grid[jax.random.permutation(jax.random.fold_in(own, 1), rows)]
    turn = jax.random.randint(jax.random.fold_in(own, 2), (rows, 1), 0, top)
    return jnp.take_along_axis(grid, (jnp.arange(top)[None, :] + turn) % top, axis=1)


def load_shares(count, total, reach, skew, full):
    loads = [(1 << 20) // math.isqrt(grade ** skew) + 1 for grade in range(1, count + 1)]
    largest = reach if full else min(reach, max(-(-total // count), total * loads[0] // sum(loads)))
    least = 1 if total - largest >= count - 1 else 0
    given, rest = [largest] + [least] * (count - 1), total - largest - least * (count - 1)
    while rest > 0:
        candidates = [i for i in range(1, count) if given[i] < largest] or [i for i in range(1, count) if given[i] < reach]
        pool, remaining = sum([loads[i] for i in candidates]), rest
        for i in candidates:
            more = min(reach - given[i], max(1, remaining * loads[i] // pool), rest)
            given[i] = given[i] + more
            rest = rest - more
    return np.array(given)


def centred(key, shape, scale, most, cuts=(), kind=jnp.bfloat16):
    entries = jax.random.normal(key, shape, jnp.float32) * scale
    if len(cuts) > 0:
        entries = level_of(key, shape, cuts, -0.22, 0.18) * entries
    return jnp.clip(entries, min=-most, max=most).astype(kind)


def noise_with(key, extent, width, bound, pieces, heavy, kind=jnp.bfloat16):
    drawn = width * jax.random.normal(key, extent, jnp.float32)
    if pieces:
        drawn = drawn * level_of(key, extent, pieces, -0.22, 0.18)
    return jnp.clip(with_spikes(drawn, jax.random.fold_in(key, 3), *heavy), -bound, bound).astype(kind)


def setup_inputs(seed: int = 0) -> dict:
    keys = jax.random.split(jax.random.key(seed), 18)
    q_latent = centred(keys[0], (TOK_A, QLAT), 1.0, 6.0, ((0, 8),))
    kv_latent = centred(keys[1], (TOK_A, KVLAT), 1.0, 6.0, ((0, 8),))
    rope_key = draw_rope_key(jax.random.fold_in(keys[17], 71), 0)
    q_gain = jnp.clip(1.0 + 0.18 * jax.random.normal(keys[3], (QLAT,), jnp.float32), 0.099609375, 1.8984375).astype(jnp.bfloat16)
    kv_gain = jnp.clip(1.0 + 0.18 * jax.random.normal(keys[4], (KVLAT,), jnp.float32), 0.099609375, 1.8984375).astype(jnp.bfloat16)
    w_q_nope = centred(keys[5], (QLAT, HEADS * NOPE), QLAT ** -0.5, 0.25, ((1, 4),))
    w_q_rope = centred(keys[6], (QLAT, HEADS * ROPE), QLAT ** -0.5, 0.25, ((1, 4),))
    w_k_nope = centred(keys[7], (KVLAT, HEADS * NOPE), KVLAT ** -0.5, 0.375, ((1, 4),))
    w_value = centred(keys[8], (KVLAT, HEADS * VDIM), KVLAT ** -0.5, 0.375, ((1, 4),))
    w_out = centred(keys[9], (HEADS * VDIM, D), 0.9, 5.375, ((0, 4),))
    tokens_b = centred(keys[10], (TOK_B, D), 1.0, 6.0, ((0, 8),))
    norm_gain_b = jnp.clip(1.0 + 0.18 * jax.random.normal(keys[11], (D,), jnp.float32), 0.099609375, 1.8984375).astype(jnp.bfloat16)
    routes_keys = jax.random.split(jax.random.fold_in(keys[12], 1), TOK_B // R_B)
    routes_turns = jax.random.permutation(jax.random.fold_in(keys[12], 3), TOK_B // R_B)
    routes = jax.vmap(lambda own, number: assign_block(jax.random.fold_in(keys[12], 2), own, number, R_B, EXPERTS, 2, CAP, 2))(routes_keys, routes_turns).reshape((TOK_B, 2))
    route_logits = centred(keys[13], (TOK_B, 2), 1.5, 6.0, ((0, 8),), jnp.float32)
    w_gate = centred(keys[14], (EXPERTS, D, FFE), D ** -0.5, 0.125, ((0, 8), (2, 4)))
    w_up = centred(keys[15], (EXPERTS, D, FFE), D ** -0.5, 0.125, ((0, 8), (2, 4)))
    w_down = noise_with(keys[16], (EXPERTS, FFE, D), FFE ** -0.5, 0.125, ((0, 8), (1, 4)), (1, 2, 4, 2.0))
    return dict(q_latent=q_latent, kv_latent=kv_latent, rope_key=rope_key, q_gain=q_gain, kv_gain=kv_gain, w_q_nope=w_q_nope, w_q_rope=w_q_rope, w_k_nope=w_k_nope, w_value=w_value, w_out=w_out, tokens_b=tokens_b, norm_gain_b=norm_gain_b, routes=routes, route_logits=route_logits, w_gate=w_gate, w_up=w_up, w_down=w_down)


EPSILON = 1e-06

def rms_rows(values, gain):
    wide = values.astype(jnp.float32)
    scaled = wide * lax.rsqrt(lax.optimization_barrier(jnp.mean(wide * wide, axis=-1, keepdims=True)) + EPSILON)
    return (scaled * gain.astype(jnp.float32)).astype(jnp.bfloat16)

def rotate(values, places):
    half = values.shape[-1] // 2
    freqs = 10000.0 ** (-jnp.arange(half, dtype=jnp.float32) / half)
    angles = places.astype(jnp.float32)[:, None] * freqs[None, :]
    cosine = jnp.cos(angles)[:, None, :]
    sine = jnp.sin(angles)[:, None, :]
    first = values[..., :half]
    second = values[..., half:]
    return jnp.concatenate([first * cosine - second * sine, first * sine + second * cosine], axis=-1)

def add_group(acc, operands):
    part = jnp.dot(operands[0], operands[1], preferred_element_type=jnp.float32).astype(jnp.bfloat16)
    part = lax.optimization_barrier(part)
    return (acc + part.astype(jnp.float32), None)

def reference(q_latent, kv_latent, rope_key, q_gain, kv_gain, w_q_nope, w_q_rope, w_k_nope, w_value, w_out, tokens_b, norm_gain_b, routes, route_logits, w_gate, w_up, w_down):
    total = q_latent.shape[0]
    places = jnp.arange(total, dtype=jnp.int32)
    q_normed = rms_rows(q_latent, q_gain)
    q_nope = jnp.dot(q_normed, w_q_nope, preferred_element_type=jnp.float32).astype(jnp.bfloat16)
    q_nope = q_nope.reshape(total, HEADS, NOPE)
    q_turn = jnp.dot(q_normed, w_q_rope, preferred_element_type=jnp.float32).reshape(total, HEADS, ROPE)
    q_rope = rotate(q_turn, places).astype(jnp.bfloat16)
    kv_normed = rms_rows(kv_latent, kv_gain)
    k_nope = jnp.dot(kv_normed, w_k_nope, preferred_element_type=jnp.float32).astype(jnp.bfloat16)
    k_nope = k_nope.reshape(total, HEADS, NOPE)
    values = jnp.dot(kv_normed, w_value, preferred_element_type=jnp.float32).astype(jnp.bfloat16)
    values = values.reshape(total, HEADS, VDIM)
    k_rope = rotate(rope_key.astype(jnp.float32)[:, None, :], places)[:, 0].astype(jnp.bfloat16)
    scale = (NOPE + ROPE) ** (-0.5)

    def one_head(operands):
        head_q, head_r, head_k, head_v = operands
        scores = jnp.dot(head_q, head_k.T, preferred_element_type=jnp.float32)
        scores = (scores + jnp.dot(head_r, k_rope.T, preferred_element_type=jnp.float32)) * scale
        top = lax.optimization_barrier(jnp.max(scores, axis=-1, keepdims=True))
        weights = jnp.exp(scores - top)
        total_w = lax.optimization_barrier(jnp.sum(weights, axis=-1, keepdims=True))
        mixed = jnp.dot(weights.astype(jnp.bfloat16), head_v, preferred_element_type=jnp.float32) / total_w
        return mixed.astype(jnp.bfloat16)
    heads_out = lax.map(one_head, (q_nope.transpose(1, 0, 2), q_rope.transpose(1, 0, 2), k_nope.transpose(1, 0, 2), values.transpose(1, 0, 2)))
    group = HEADS // N_TP
    grouped = heads_out.reshape(N_TP, group, total, VDIM).transpose(0, 2, 1, 3).reshape(N_TP, total, group * VDIM)
    out_rows = w_out.reshape(N_TP, group * VDIM, D)
    summed, _ = lax.scan(add_group, jnp.zeros((total, D), jnp.float32), (grouped, out_rows))
    mixer_out = summed.astype(jnp.bfloat16)
    rows_b = tokens_b.shape[0]
    normed_b = rms_rows(tokens_b, norm_gain_b)
    weights_b = jax.nn.softmax(route_logits.astype(jnp.float32), axis=-1)
    flat = routes.reshape(-1).astype(jnp.int32)
    assigned = flat.shape[0]
    onehot = (flat[:, None] == jnp.arange(EXPERTS, dtype=jnp.int32)[None, :]).astype(jnp.int32)
    slot = lax.optimization_barrier(jnp.sum((jnp.cumsum(onehot, axis=0) - 1) * onehot, axis=1)).astype(jnp.int32)
    room = N_EP * CAP
    table = jnp.full((EXPERTS, room), assigned, jnp.int32).at[flat, slot].set(jnp.arange(assigned, dtype=jnp.int32))
    padded = jnp.concatenate([normed_b, jnp.zeros((1, D), jnp.bfloat16)], axis=0)
    slices = FFE // N_TP

    def one_expert(operands):
        picks, gate_w, up_w, down_w = operands
        rows = padded[picks // 2]
        gate = jnp.dot(rows, gate_w, preferred_element_type=jnp.float32)
        up = jnp.dot(rows, up_w, preferred_element_type=jnp.float32)
        hidden = (jax.nn.silu(gate) * up).astype(jnp.bfloat16)
        hidden = hidden.reshape(room, N_TP, slices).transpose(1, 0, 2)
        down = down_w.reshape(N_TP, slices, D)
        total_e, _ = lax.scan(add_group, jnp.zeros((room, D), jnp.float32), (hidden, down))
        return total_e.astype(jnp.bfloat16)
    expert_out = lax.map(one_expert, (table, w_gate, w_up, w_down)).reshape(EXPERTS * room, D)
    where = (flat * room + slot).reshape(rows_b, 2)
    picked = expert_out[where].astype(jnp.float32)
    expert_mix = lax.optimization_barrier(jnp.sum(picked * weights_b[:, :, None], axis=1)).astype(jnp.bfloat16)
    return (mixer_out, expert_mix)
```

```python
import functools
import math

import jax
import jax.numpy as jnp
import numpy as np
from jax import lax
from jax.experimental import pallas as pl
from jax.experimental.pallas import tpu as pltpu
from jax.sharding import PartitionSpec as P

NOPE = 64
ROPE = 32
VDIM = 64
LANES = 128
BAND = 16
EPSILON = 1e-06
BF = jnp.bfloat16
F32 = jnp.float32
MESH = pl.DeviceIdType.MESH


def rms_rows(values, gain):
    wide = values.astype(F32)
    scaled = wide * lax.rsqrt(jnp.mean(wide * wide, axis=-1, keepdims=True) + EPSILON)
    return (scaled * gain.astype(F32)).astype(BF)


def remote(src, dst, send, recv, ep, tp):
    return pltpu.make_async_remote_copy(
        src_ref=src,
        dst_ref=dst,
        send_sem=send,
        recv_sem=recv,
        device_id={"ep": ep, "tp": tp},
        device_id_type=MESH,
    )


def loop(count, body, start=0):
    def step(i, c):
        body(i)
        return c

    lax.fori_loop(start, count, step, 0)


class Spread:
    def __init__(self, count, n_tp, ep, t, view, index, recv, send, sib=None):
        self.count, self.n_tp, self.ep, self.t = count, n_tp, ep, t
        self.view, self.index, self.recv, self.send = view, index, recv, send
        self.square = n_tp == 4
        self.direct = 3 if self.square else n_tp
        self.sib = sib

    def at(self, d):
        if self.square:
            return (self.t // 2 + d // 2) % 2 * 2 + (self.t % 2 + d % 2) % 2
        return (self.t + d) % self.n_tp

    def frm(self, d):
        return self.at(d) if self.square else (self.t + self.n_tp - d) % self.n_tp

    def copy(self, i, d):
        ref = self.view(i, self.t)
        sem = self.recv.at[self.index(i, self.t)]
        return remote(ref, ref, self.send.at[i * self.n_tp + d], sem, self.ep, self.at(d))

    def passed(self, i):
        owner = self.at(1 + i % 2)
        ref = self.view(i, owner)
        sem = self.recv.at[self.index(i, owner)]
        return remote(ref, ref, self.send.at[i * self.n_tp + 3], sem, self.ep, self.at(2 - i % 2))

    def across(self, i, d):
        owner = self.frm(d)
        ref = self.view(i, owner)
        recv, send = self.sib
        sem = recv.at[self.index(i, owner)]
        return remote(ref, ref, send.at[i * self.n_tp + d], sem, self.ep // 2 * 2 + 1 - self.ep % 2, self.t)

    def landed(self, i, d):
        owner = self.frm(d)
        ref = self.view(i, owner)
        remote(ref, ref, self.send.at[0], self.recv.at[self.index(i, owner)], self.ep, self.t).wait_recv()

    def push(self, i):
        loop(self.direct, lambda d: self.copy(i, d).start(), 1)

    def relay(self, i):
        def one(d):
            self.landed(i, d)
            if self.sib is not None:
                self.across(i, d).start()

        loop(self.direct, one, 1)
        if self.square:
            self.passed(i).start()

    def last(self, i):
        if self.square:
            self.landed(i, 3)
            if self.sib is not None:
                self.across(i, 3).start()

    def drain(self, i, first=1):
        loop(self.direct, lambda d: self.copy(i, d).wait_send(), 1)
        if self.square:
            self.passed(i).wait_send()
        if self.sib is not None:
            loop(self.n_tp, lambda d: self.across(i, d).wait_send(), first)


def mega_kernel(
    heads,
    n_ep,
    n_tp,
    kv_ref,
    rope_ref,
    lat_ref,
    qg_ref,
    kvg_ref,
    bg_ref,
    cosb_ref,
    sinb_ref,
    cosa_ref,
    sina_ref,
    qn_ref,
    qr_ref,
    wk_ref,
    wv_ref,
    tokb_ref,
    route_ref,
    logit_ref,
    wo_hbm,
    wg_hbm,
    wu_hbm,
    wd_hbm,
    mix_ref,
    exp_ref,
    wo,
    wg,
    wu,
    wd,
    kv_buf,
    k_buf,
    v_buf,
    q_ref,
    w_ref,
    acc_ref,
    top_ref,
    att_ref,
    a_buf,
    x_send,
    x_recv,
    hid,
    t_send,
    t_recv,
    e_send,
    e_recv,
    own_hi,
    own_lo,
    w_sem,
    lat_zs,
    lat_ts,
    lat_cs,
    lat_recv,
    lat_own,
    x_zs,
    x_ts,
    x_recv_sem,
    x_own,
    wo_ts,
    wo_recv,
    wo_cs,
    wo_crecv,
    as_,
    ar,
    ts,
    tr,
    es,
    er,
):
    ep, t = lax.axis_index("ep"), lax.axis_index("tp")
    nz = n_ep // 2
    z, core = ep // 2, ep % 2
    sibling = z * 2 + 1 - core
    rows, deep = lat_ref.shape
    lat = wk_ref.shape[0]
    unit = kv_buf.shape[2]
    part = rows // n_tp
    room, width = x_send.shape[1:]
    share = width // n_tp
    rows_b = tokb_ref.shape[0]
    depth = wo.shape[1]
    pieces = wo_ts.shape[0] // n_tp
    slab = depth // 2 // pieces
    half = ROPE // 2
    scale = (NOPE + ROPE) ** (-0.5) * math.log2(math.e)
    wide = heads * LANES

    loads = [
        pltpu.make_async_copy(a, b, w_sem.at[i])
        for i, (a, b) in enumerate(((wo_hbm, wo.at[t]), (wg_hbm, wg), (wu_hbm, wu), (wd_hbm, wd)))
    ]
    for load in loads:
        load.start()

    barrier = pltpu.get_barrier_semaphore()

    def hello(e, tp):
        pl.semaphore_signal(barrier, inc=1, device_id={"ep": e, "tp": tp}, device_id_type=MESH)

    loop(n_tp, lambda d: hello(ep, (t + d) % n_tp), 1)
    loop(n_ep, lambda d: hello((ep + d) % n_ep, t), 1)

    def columns(s):
        return pl.ds(pl.multiple_of(s * share, share), share)

    def plane(d):
        return (z + d) % nz

    slots = n_ep * room
    lane = lax.broadcasted_iota(jnp.int32, (rows_b, slots), 1)
    expert = jnp.floor((lane.astype(F32) + 0.5) * (1.0 / room))
    place = lane.astype(F32) - expert * room
    first = route_ref[:, :1].astype(F32) == expert
    second = route_ref[:, 1:2].astype(F32) == expert
    named = (first | second).astype(F32)
    r = lax.broadcasted_iota(jnp.int32, (rows_b, rows_b), 0)
    c = lax.broadcasted_iota(jnp.int32, (rows_b, rows_b), 1)
    ahead = jnp.dot((c < r).astype(F32).astype(BF), named.astype(BF), preferred_element_type=F32)
    mine = jnp.where(ahead == place, named, 0.0)
    logits = logit_ref[...]
    peak = jnp.max(logits, axis=-1, keepdims=True)
    grown = jnp.exp(logits - peak)
    weights = grown / jnp.sum(grown, axis=-1, keepdims=True)
    weighted = mine * jnp.where(first, weights[:, :1], weights[:, 1:2])
    high = weighted.astype(BF)
    own_hi[...] = high
    own_lo[...] = (weighted - high.astype(F32)).astype(BF)

    normed_b = rms_rows(tokb_ref[...], bg_ref[...])
    pick = jnp.transpose(mine).astype(BF)
    span = min(512, width)
    for s in range(width // span):
        got = jnp.dot(pick, normed_b[:, s * span : (s + 1) * span], preferred_element_type=F32)
        x_send[:, :, s * span : (s + 1) * span] = got.astype(BF).reshape(n_ep, room, span)
    x_recv[ep] = x_send[ep]

    cos_a, sin_a = cosa_ref[pl.ds(ep, 1), :], sina_ref[pl.ds(ep, 1), :]
    cos = cos_a * cosb_ref[...] - sin_a * sinb_ref[...]
    sin = sin_a * cosb_ref[...] + cos_a * sinb_ref[...]
    normed_kv = rms_rows(kv_ref[...], kvg_ref[...])
    raw = rope_ref[...].astype(F32)
    front = jnp.zeros((rows, NOPE), F32)
    back = jnp.zeros((rows, LANES - NOPE - ROPE), F32)
    plain = jnp.concatenate([front, raw, back], axis=1)
    turned = jnp.concatenate([front, -raw[:, half:], raw[:, :half], back], axis=1)
    rot = plain * cos + turned * sin
    for s in range(n_tp):
        kv_buf[ep, s, :part, :] = normed_kv[s * part : (s + 1) * part]
        bands = [jnp.zeros((BAND, LANES), F32)] * ((unit - part) // BAND * 2)
        for g in range(part // BAND):
            at = s * part + g * BAND
            shift = (32 * (g % 4) - NOPE) % LANES
            piece = rot[at : at + BAND]
            bands[g // 4] = bands[g // 4] + (pltpu.roll(piece, shift, 1) if shift else piece)
        for b in range(len(bands) // 2):
            pair = jnp.concatenate(bands[2 * b : 2 * b + 2], axis=1).astype(BF)
            kv_buf[ep, s, part + b * BAND : part + (b + 1) * BAND, :] = pair

    pl.semaphore_wait(barrier, n_tp + n_ep - 2)

    def x_to(i):
        to = plane(1 + i // 2) * 2 + i % 2
        at = columns(t)
        return remote(
            x_send.at[to, :, at],
            x_recv.at[ep, :, at],
            x_zs.at[i],
            x_recv_sem.at[ep * n_tp + t],
            to,
            t,
        )

    def x_from(i):
        return plane(1 + i // 2) * 2 + i % 2

    routed = Spread(
        n_ep - 2,
        n_tp,
        ep,
        t,
        lambda i, s: x_recv.at[x_from(i), :, columns(s)],
        lambda i, s: x_from(i) * n_tp + s,
        x_recv_sem,
        x_ts,
    )
    x_beside = remote(x_send.at[sibling], x_recv.at[ep], x_own.at[0], x_own.at[1], sibling, t)

    def l_to(d):
        mine = kv_buf.at[ep, t]
        return remote(mine, mine, lat_zs.at[d], lat_recv.at[ep * n_tp + t], plane(d) * 2 + core, t)

    def l_from(i):
        return plane(1 + i) * 2 + core

    latents = Spread(
        nz - 1,
        n_tp,
        ep,
        t,
        lambda i, s: kv_buf.at[l_from(i), s],
        lambda i, s: l_from(i) * n_tp + s,
        lat_recv,
        lat_ts,
        (lat_recv, lat_cs),
    )
    l_beside = remote(kv_buf.at[ep], kv_buf.at[ep], lat_own.at[0], lat_own.at[1], sibling, t)

    projection = Spread(
        pieces,
        n_tp,
        ep,
        t,
        lambda i, s: wo.at[s, pl.ds(pl.multiple_of((core * pieces + i) * slab, slab), slab), :],
        lambda i, s: i * n_tp + s,
        wo_recv,
        wo_ts,
        (wo_crecv, wo_cs),
    )

    l_beside.start()
    x_beside.start()
    loop(n_ep - 2, lambda i: x_to(i).start())
    loop(nz, lambda d: l_to(d).start(), 1)
    loads[0].wait()
    projection.push(0)

    def beside(parts, height, filled):
        filler = jnp.zeros((height, LANES - filled), BF)
        return jnp.concatenate(parts + [filler], axis=1)

    for h in range(heads):
        nope, value = slice(h * NOPE, (h + 1) * NOPE), slice(h * VDIM, (h + 1) * VDIM)
        w_ref[:, h * LANES : (h + 1) * LANES] = beside([wk_ref[:, nope]], lat, NOPE)
        w_ref[:, wide + h * LANES : wide + (h + 1) * LANES] = beside([wv_ref[:, value]], lat, VDIM)
    normed = rms_rows(lat_ref[...], qg_ref[...])
    for h in range(heads):
        turn = qr_ref[:, h * ROPE : (h + 1) * ROPE]
        plain = beside([qn_ref[:, h * NOPE : (h + 1) * NOPE], turn], deep, NOPE + ROPE)
        blank = jnp.zeros((deep, NOPE), BF)
        turned = beside([blank, -turn[:, half:], turn[:, :half]], deep, NOPE + ROPE)
        q = jnp.dot(normed, plain, preferred_element_type=F32) * cos
        q = q + jnp.dot(normed, turned, preferred_element_type=F32) * sin
        q_ref[h] = q.astype(BF)

    keys = 2 * rows
    q_block = min(256, rows)

    def project(d):
        for j in range(2):
            block = kv_buf[plane(d) * 2 + j]
            tall = block[:, :part, :].reshape(rows, lat)
            up = jnp.dot(tall, w_ref[...], preferred_element_type=F32)
            pieces_ = []
            for s in range(n_tp):
                packed = block[s, part:, :].astype(F32)
                for g in range(part // BAND):
                    b, q = g // 8, g % 8 // 4
                    piece = packed[b * BAND : (b + 1) * BAND, q * LANES : (q + 1) * LANES]
                    shift = (NOPE - 32 * (g % 4)) % LANES
                    pieces_.append(pltpu.roll(piece, shift, 1) if shift else piece)
            turned = jnp.concatenate(pieces_, axis=0)
            spot = lax.broadcasted_iota(jnp.int32, (rows, LANES), 1)
            turned = jnp.where((spot >= NOPE) & (spot < NOPE + ROPE), turned, 0.0)
            at = slice(j * rows, (j + 1) * rows)
            for h in range(heads):
                k_buf[h, at, :] = (up[:, h * LANES : (h + 1) * LANES] + turned).astype(BF)
                v = up[:, wide + h * LANES : wide + (h + 1) * LANES]
                v_buf[h, at, :] = jnp.where(spot < VDIM, v, 1.0).astype(BF)

    def attend(h, step, start):
        here = pl.ds(step * q_block if isinstance(step, int) else pl.multiple_of(step * q_block, q_block), q_block)
        s = lax.dot_general(
            q_ref[h, here, :], k_buf[h], (((1,), (1,)), ((), ())), preferred_element_type=F32
        )
        top = jnp.max(s, axis=-1, keepdims=True)
        if not start:
            old = top_ref[h, here, :1]
            top = jnp.maximum(old, top)
        p = jnp.exp2((s - top) * scale).astype(BF)
        pv = jnp.dot(p, v_buf[h], preferred_element_type=F32)
        if not start:
            pv = acc_ref[h, here, :] * jnp.exp2((old - top) * scale) + pv
        acc_ref[h, here, :] = pv
        top_ref[h, here, :] = jnp.broadcast_to(top, (q_block, LANES))

    def attend_all(start):
        def step(i):
            for h in range(heads):
                attend(h, i, start)

        loop(rows // q_block, step)

    l_beside.wait_recv()
    project(0)
    attend_all(True)
    loop(n_ep - 2, lambda i: (routed.landed(i, 0), routed.push(i)))
    loop(nz - 1, lambda i: (latents.landed(i, 0), latents.push(i), latents.across(i, 0).start()))
    loop(n_ep - 2, routed.relay)
    loop(nz - 1, latents.relay)
    loop(pieces, projection.push, 1)
    x_beside.wait_recv()
    loop(n_ep - 2, routed.last)

    step = min(256, hid.shape[1])
    loads[1].wait()
    loads[2].wait()
    total = n_ep * room

    def up(i):
        at = pl.ds(pl.multiple_of(i * step, step), step)
        x = x_recv[...].reshape(total, width)
        g = jnp.dot(x, wg[:, at], preferred_element_type=F32)
        u = jnp.dot(x, wu[:, at], preferred_element_type=F32)
        hid[:, at] = (g / (1.0 + jnp.exp(-g)) * u).astype(BF)

    loop(hid.shape[1] // step, up)
    loads[3].wait()
    loop(nz - 1, latents.last)

    def to_tp(src, recv, ss, rs, d):
        return remote(src, recv.at[t], ss.at[d], rs.at[t], ep, (t + d) % n_tp)

    def from_tp(recv, ss, rs, d):
        frm = (t + n_tp - d) % n_tp
        remote(recv.at[frm], recv.at[frm], ss.at[0], rs.at[frm], ep, frm).wait_recv()
        return frm

    def term(d):
        return to_tp(t_send.at[(t + d) % n_tp], t_recv, ts, tr, d)

    def down(d):
        to = (t + d) % n_tp
        t_send[to] = jnp.dot(hid[...], wd[:, columns(to)], preferred_element_type=F32).astype(BF)

        @pl.when(d < n_tp)
        def _():
            term(d).start()

    loop(n_tp + 1, down, 1)

    def other(i):
        def beside_landed(s):
            at = plane(1 + i) * 2 + 1 - core
            ref = kv_buf.at[at, s]
            remote(ref, ref, lat_own.at[0], lat_recv.at[at * n_tp + s], sibling, t).wait_recv()

        loop(n_tp, beside_landed)
        project(1 + i)
        attend_all(False)

    def to_ep(d):
        to = (ep + d) % n_ep
        return remote(e_send.at[to], e_recv.at[ep], es.at[d], er.at[ep], to, t)

    def give_back():
        out = t_send[t].astype(F32)
        for d in range(1, n_tp):
            out = out + t_recv[from_tp(t_recv, ts, tr, d)].astype(F32)
        e_send[...] = out.astype(BF).reshape(n_ep, room, share)
        e_recv[ep] = e_send[ep]
        loop(n_ep, lambda d: to_ep(d).start(), 1)

    def tail(i):
        other(i)

        @pl.when(i == 0)
        def _():
            loop(pieces, projection.relay)

    loop(nz - 1, tail)
    loop(pieces, projection.last)

    def finish(i):
        here = pl.ds(pl.multiple_of(i * q_block, q_block), q_block)
        done = []
        for h in range(heads):
            acc = acc_ref[h, here, :]
            done.append((acc[:, :VDIM] / acc[:, VDIM : VDIM + 1]).astype(BF))
        att_ref[here, :] = done[0] if heads == 1 else jnp.concatenate(done, axis=1)

    loop(rows // q_block, finish)

    def piece_of(s):
        return pl.ds(pl.multiple_of(s * part, part), part)

    def attended(d):
        return to_tp(att_ref.at[piece_of((t + d) % n_tp), :], a_buf, as_, ar, d)

    loop(n_tp, lambda d: attended(d).start(), 1)
    a_buf[t] = att_ref[piece_of(t), :]
    give_back()

    def across_landed(i):
        def one(d):
            owner = projection.frm(d)
            at = pl.ds(pl.multiple_of(((1 - core) * pieces + i) * slab, slab), slab)
            ref = wo.at[owner, at, :]
            remote(ref, ref, wo_cs.at[0], wo_crecv.at[i * n_tp + owner], sibling, t).wait_recv()

        loop(n_tp, one, 1)

    loop(pieces, across_landed)
    for d in range(1, n_tp):
        from_tp(a_buf, as_, ar, d)

    def mix(s):
        at = pl.ds(pl.multiple_of(s * span, span), span)
        out = jnp.zeros((part, span), F32)
        for g in range(n_tp):
            out = out + jnp.dot(a_buf[g], wo[g, :, at], preferred_element_type=F32)
        mix_ref[:, at] = out.astype(BF)

    loop(width // span, mix)

    def arrived(d):
        frm = (ep + n_ep - d) % n_ep
        remote(e_recv.at[frm], e_recv.at[frm], es.at[0], er.at[frm], frm, t).wait_recv()

    loop(n_ep, arrived, 1)
    home = e_recv[...].reshape(total, share)
    out = jnp.dot(own_hi[...], home, preferred_element_type=F32)
    out = out + jnp.dot(own_lo[...], home, preferred_element_type=F32)
    exp_ref[...] = out.astype(BF)

    l_beside.wait_send()
    x_beside.wait_send()
    loop(n_ep - 2, lambda i: (x_to(i).wait_send(), routed.drain(i)))
    loop(nz, lambda d: l_to(d).wait_send(), 1)
    loop(nz - 1, lambda i: latents.drain(i, 0))
    loop(pieces, projection.drain)
    loop(n_tp, lambda d: (term(d).wait_send(), attended(d).wait_send()), 1)
    loop(n_ep, lambda d: to_ep(d).wait_send(), 1)


def turn_tables(n_ep, rows):
    half = ROPE // 2
    freqs = 10000.0 ** (-np.arange(half) / half)
    lanes = np.zeros(LANES)
    lanes[NOPE : NOPE + half] = freqs
    lanes[NOPE + half : NOPE + ROPE] = freqs
    near = np.arange(rows)[:, None] * lanes
    far = (np.arange(n_ep) * rows)[:, None] * lanes
    return [f(a).astype(np.float32) for a in (near, far) for f in (np.cos, np.sin)]


def mega(n_ep, n_tp, heads, operands, w_out, w_gate, w_up, w_down):
    kv, rope, latent = operands[:3]
    tokens = operands[14]
    rows = latent.shape[0]
    rows_b, width = tokens.shape
    lat = kv.shape[1]
    part = rows // n_tp
    unit = part + -(-part // LANES) * BAND
    room = -(-(3 * rows_b // n_ep) // BAND) * BAND
    total = n_ep * room
    share = width // n_tp
    hidden = w_gate.shape[1]
    nz = n_ep // 2
    depth = w_out.shape[0]
    pieces = min(4, depth // 2 // BAND)
    vmem = pl.BlockSpec(memory_space=pltpu.VMEM)
    hbm = pl.BlockSpec(memory_space=pl.ANY)
    dma = pltpu.SemaphoreType.DMA
    keys = rows * n_ep
    flops = 4 * heads * rows * keys * 256 + 6 * total * width * hidden
    return pl.pallas_call(
        functools.partial(mega_kernel, heads, n_ep, n_tp),
        out_shape=(
            jax.ShapeDtypeStruct((part, width), BF),
            jax.ShapeDtypeStruct((rows_b, share), BF),
        ),
        in_specs=[vmem] * len(operands) + [hbm] * 4,
        out_specs=(vmem, vmem),
        scratch_shapes=[
            pltpu.VMEM((n_tp,) + w_out.shape, BF),
            pltpu.VMEM(w_gate.shape, BF),
            pltpu.VMEM(w_up.shape, BF),
            pltpu.VMEM(w_down.shape, BF),
            pltpu.VMEM((n_ep, n_tp, unit, lat), BF),
            pltpu.VMEM((heads, 2 * rows, LANES), BF),
            pltpu.VMEM((heads, 2 * rows, LANES), BF),
            pltpu.VMEM((heads, rows, LANES), BF),
            pltpu.VMEM((lat, 2 * heads * LANES), BF),
            pltpu.VMEM((heads, rows, LANES), F32),
            pltpu.VMEM((heads, rows, LANES), F32),
            pltpu.VMEM((rows, heads * VDIM), BF),
            pltpu.VMEM((n_tp, part, heads * VDIM), BF),
            pltpu.VMEM((n_ep, room, width), BF),
            pltpu.VMEM((n_ep, room, width), BF),
            pltpu.VMEM((total, hidden), BF),
            pltpu.VMEM((n_tp, total, share), BF),
            pltpu.VMEM((n_tp, total, share), BF),
            pltpu.VMEM((n_ep, room, share), BF),
            pltpu.VMEM((n_ep, room, share), BF),
            pltpu.VMEM((rows_b, total), BF),
            pltpu.VMEM((rows_b, total), BF),
            dma((4,)),
            dma((nz,)),
            dma((nz * n_tp,)),
            dma((nz * n_tp,)),
            dma((n_ep * n_tp,)),
            dma((2,)),
            dma((n_ep,)),
            dma((n_ep * n_tp,)),
            dma((n_ep * n_tp,)),
            dma((2,)),
            dma((pieces * n_tp,)),
            dma((pieces * n_tp,)),
            dma((pieces * n_tp,)),
            dma((pieces * n_tp,)),
            dma((n_tp,)),
            dma((n_tp,)),
            dma((n_tp,)),
            dma((n_tp,)),
            dma((n_ep,)),
            dma((n_ep,)),
        ],
        compiler_params=pltpu.CompilerParams(
            vmem_limit_bytes=60 * 1024 * 1024, collective_id=0, has_side_effects=True
        ),
        cost_estimate=pl.CostEstimate(
            flops=flops, bytes_accessed=20 * 1024 * 1024, transcendentals=heads * rows * keys
        ),
        name="mega",
    )(*operands, w_out, w_gate, w_up, w_down)


def shards(
    q_latent,
    kv_latent,
    rope_key,
    q_gain,
    kv_gain,
    w_q_nope,
    w_q_rope,
    w_k_nope,
    w_value,
    w_out,
    tokens_b,
    norm_gain_b,
    routes,
    route_logits,
    w_gate,
    w_up,
    w_down,
):
    n_ep = lax.axis_size("ep")
    n_tp = lax.axis_size("tp")
    heads = w_q_nope.shape[1] // NOPE
    cos_b, sin_b, cos_a, sin_a = turn_tables(n_ep, q_latent.shape[0])
    operands = (
        kv_latent,
        rope_key,
        q_latent,
        q_gain[None, :],
        kv_gain[None, :],
        norm_gain_b[None, :],
        cos_b,
        sin_b,
        cos_a,
        sin_a,
        w_q_nope,
        w_q_rope,
        w_k_nope,
        w_value,
        tokens_b,
        routes,
        route_logits,
    )
    return mega(n_ep, n_tp, heads, operands, w_out, w_gate[0], w_up[0], w_down[0])


def solution(mesh):
    placed = (
        P("ep", None),
        P("ep", None),
        P("ep", None),
        P(),
        P(),
        P(None, "tp"),
        P(None, "tp"),
        P(None, "tp"),
        P(None, "tp"),
        P("tp", None),
        P("ep", None),
        P(),
        P("ep", None),
        P("ep", None),
        P("ep", None, "tp"),
        P("ep", None, "tp"),
        P("ep", "tp", None),
    )
    return jax.shard_map(
        shards,
        mesh=mesh,
        in_specs=placed,
        out_specs=(P(("ep", "tp"), None), P("ep", "tp")),
        check_vma=False,
    )
```

```python
import functools
import math

import jax
import jax.numpy as jnp
import numpy as np
from jax import lax
from jax.experimental import pallas as pl
from jax.experimental.pallas import tpu as pltpu
from jax.sharding import PartitionSpec as P

NOPE = 64
ROPE = 32
VDIM = 64
LANES = 128
BAND = 16
EPSILON = 1e-06
BF = jnp.bfloat16
F32 = jnp.float32
MESH = pl.DeviceIdType.MESH


def rms_rows(values, gain):
    wide = values.astype(F32)
    scaled = wide * lax.rsqrt(jnp.mean(wide * wide, axis=-1, keepdims=True) + EPSILON)
    return (scaled * gain.astype(F32)).astype(BF)


def remote(src, dst, send, recv, ep, tp):
    return pltpu.make_async_remote_copy(
        src_ref=src,
        dst_ref=dst,
        send_sem=send,
        recv_sem=recv,
        device_id={"ep": ep, "tp": tp},
        device_id_type=MESH,
    )


def loop(count, body, start=0):
    def step(i, c):
        body(i)
        return c

    lax.fori_loop(start, count, step, 0)


class Spread:
    def __init__(self, count, n_tp, ep, t, view, index, recv, send, sib=None):
        self.count, self.n_tp, self.ep, self.t = count, n_tp, ep, t
        self.view, self.index, self.recv, self.send = view, index, recv, send
        self.square = n_tp == 4
        self.direct = 3 if self.square else n_tp
        self.sib = sib

    def at(self, d):
        if self.square:
            return (self.t // 2 + d // 2) % 2 * 2 + (self.t % 2 + d % 2) % 2
        return (self.t + d) % self.n_tp

    def frm(self, d):
        return self.at(d) if self.square else (self.t + self.n_tp - d) % self.n_tp

    def copy(self, i, d):
        ref = self.view(i, self.t)
        sem = self.recv.at[self.index(i, self.t)]
        return remote(ref, ref, self.send.at[i * self.n_tp + d], sem, self.ep, self.at(d))

    def passed(self, i):
        owner = self.at(1 + i % 2)
        ref = self.view(i, owner)
        sem = self.recv.at[self.index(i, owner)]
        return remote(ref, ref, self.send.at[i * self.n_tp + 3], sem, self.ep, self.at(2 - i % 2))

    def across(self, i, d):
        owner = self.frm(d)
        ref = self.view(i, owner)
        recv, send = self.sib
        sem = recv.at[self.index(i, owner)]
        return remote(ref, ref, send.at[i * self.n_tp + d], sem, self.ep // 2 * 2 + 1 - self.ep % 2, self.t)

    def landed(self, i, d):
        owner = self.frm(d)
        ref = self.view(i, owner)
        remote(ref, ref, self.send.at[0], self.recv.at[self.index(i, owner)], self.ep, self.t).wait_recv()

    def push(self, i):
        loop(self.direct, lambda d: self.copy(i, d).start(), 1)

    def relay(self, i):
        def one(d):
            self.landed(i, d)
            if self.sib is not None:
                self.across(i, d).start()

        loop(self.direct, one, 1)
        if self.square:
            self.passed(i).start()

    def last(self, i):
        if self.square:
            self.landed(i, 3)
            if self.sib is not None:
                self.across(i, 3).start()

    def drain(self, i, first=1):
        loop(self.direct, lambda d: self.copy(i, d).wait_send(), 1)
        if self.square:
            self.passed(i).wait_send()
        if self.sib is not None:
            loop(self.n_tp, lambda d: self.across(i, d).wait_send(), first)


def mega_kernel(
    heads,
    n_ep,
    n_tp,
    kv_ref,
    rope_ref,
    lat_ref,
    gain_ref,
    cosb_ref,
    sinb_ref,
    cosa_ref,
    sina_ref,
    qn_ref,
    qr_ref,
    wk_ref,
    wv_ref,
    tokb_ref,
    route_ref,
    logit_ref,
    wo_hbm,
    wg_hbm,
    wu_hbm,
    wd_hbm,
    mix_ref,
    exp_ref,
    wo,
    wg,
    wu,
    wd,
    kv_buf,
    k_buf,
    v_buf,
    q_ref,
    w_ref,
    acc_ref,
    top_ref,
    att_ref,
    a_buf,
    x_send,
    x_recv,
    hid,
    t_send,
    t_recv,
    e_send,
    e_recv,
    own_hi,
    own_lo,
    w_sem,
    lat_zs,
    lat_ts,
    lat_cs,
    lat_recv,
    lat_own,
    x_zs,
    x_ts,
    x_recv_sem,
    x_own,
    wo_ts,
    wo_recv,
    wo_cs,
    wo_crecv,
    as_,
    ar,
    ts,
    tr,
    es,
    er,
):
    ep, t = lax.axis_index("ep"), lax.axis_index("tp")
    nz = n_ep // 2
    z, core = ep // 2, ep % 2
    sibling = z * 2 + 1 - core
    rows, deep = lat_ref.shape
    lat = wk_ref.shape[0]
    unit = kv_buf.shape[2]
    part = rows // n_tp
    room, width = x_send.shape[1:]
    share = width // n_tp
    rows_b = tokb_ref.shape[0]
    depth = wo.shape[1]
    pieces = wo_ts.shape[0] // n_tp
    slab = depth // 2 // pieces
    half = ROPE // 2
    scale = (NOPE + ROPE) ** (-0.5) * math.log2(math.e)
    wide = heads * LANES

    loads = [
        pltpu.make_async_copy(a, b, w_sem.at[i])
        for i, (a, b) in enumerate(((wo_hbm, wo.at[t]), (wg_hbm, wg), (wu_hbm, wu), (wd_hbm, wd)))
    ]
    for load in loads:
        load.start()

    barrier = pltpu.get_barrier_semaphore()

    def hello(e, tp):
        pl.semaphore_signal(barrier, inc=1, device_id={"ep": e, "tp": tp}, device_id_type=MESH)

    loop(n_tp, lambda d: hello(ep, (t + d) % n_tp), 1)
    loop(n_ep, lambda d: hello((ep + d) % n_ep, t), 1)

    def columns(s):
        return pl.ds(pl.multiple_of(s * share, share), share)

    def plane(d):
        return (z + d) % nz

    def source(d):
        return (z + nz - d) % nz

    slots = n_ep * room
    lane = lax.broadcasted_iota(jnp.int32, (rows_b, slots), 1)
    expert = jnp.floor((lane.astype(F32) + 0.5) * (1.0 / room))
    place = lane.astype(F32) - expert * room
    def standing(ref):
        return jnp.transpose(jnp.broadcast_to(ref[:1, :], (8, rows_b))), jnp.transpose(
            jnp.broadcast_to(ref[1:2, :], (8, rows_b))
        )

    route = [x[:, :1] for x in standing(route_ref[...].astype(F32))]
    first, second = route[0] == expert, route[1] == expert
    named = (first | second).astype(F32)
    r = lax.broadcasted_iota(jnp.int32, (rows_b, rows_b), 0)
    c = lax.broadcasted_iota(jnp.int32, (rows_b, rows_b), 1)
    ahead = jnp.dot((c < r).astype(F32).astype(BF), named.astype(BF), preferred_element_type=F32)
    mine = jnp.where(ahead == place, named, 0.0)
    logits = logit_ref[...]
    peak = jnp.max(logits, axis=0, keepdims=True)
    grown = jnp.exp(logits - peak)
    weights = [x[:, :1] for x in standing(grown / jnp.sum(grown, axis=0, keepdims=True))]
    weighted = mine * jnp.where(first, weights[0], weights[1])
    high = weighted.astype(BF)
    own_hi[...] = high
    own_lo[...] = (weighted - high.astype(F32)).astype(BF)

    normed_b = rms_rows(tokb_ref[...], gain_ref[:, deep + lat :])
    pick = jnp.transpose(mine).astype(BF)
    span = min(512, width)
    for s in range(width // span):
        got = jnp.dot(pick, normed_b[:, s * span : (s + 1) * span], preferred_element_type=F32)
        x_send[:, :, s * span : (s + 1) * span] = got.astype(BF).reshape(n_ep, room, span)
    x_recv[ep] = x_send[ep]

    cos_a, sin_a = cosa_ref[pl.ds(ep, 1), :], sina_ref[pl.ds(ep, 1), :]
    cos = cos_a * cosb_ref[...] - sin_a * sinb_ref[...]
    sin = sin_a * cosb_ref[...] + cos_a * sinb_ref[...]
    normed_kv = rms_rows(kv_ref[...], gain_ref[:, deep : deep + lat])
    raw = jnp.transpose(rope_ref[...].astype(F32))
    front = jnp.zeros((rows, NOPE), F32)
    back = jnp.zeros((rows, LANES - NOPE - ROPE), F32)
    plain = jnp.concatenate([front, raw, back], axis=1)
    turned = jnp.concatenate([front, -raw[:, half:], raw[:, :half], back], axis=1)
    rot = plain * cos + turned * sin
    for s in range(n_tp):
        kv_buf[ep, s, :part, :] = normed_kv[s * part : (s + 1) * part]
        bands = [jnp.zeros((BAND, LANES), F32)] * ((unit - part) // BAND * 2)
        for g in range(part // BAND):
            at = s * part + g * BAND
            shift = (32 * (g % 4) - NOPE) % LANES
            piece = rot[at : at + BAND]
            bands[g // 4] = bands[g // 4] + (pltpu.roll(piece, shift, 1) if shift else piece)
        for b in range(len(bands) // 2):
            pair = jnp.concatenate(bands[2 * b : 2 * b + 2], axis=1).astype(BF)
            kv_buf[ep, s, part + b * BAND : part + (b + 1) * BAND, :] = pair

    pl.semaphore_wait(barrier, n_tp + n_ep - 2)

    def x_to(i):
        to = plane(1 + i // 2) * 2 + i % 2
        at = columns(t)
        return remote(
            x_send.at[to, :, at],
            x_recv.at[ep, :, at],
            x_zs.at[i],
            x_recv_sem.at[ep * n_tp + t],
            to,
            t,
        )

    def x_from(i):
        return source(1 + i // 2) * 2 + i % 2

    routed = Spread(
        n_ep - 2,
        n_tp,
        ep,
        t,
        lambda i, s: x_recv.at[x_from(i), :, columns(s)],
        lambda i, s: x_from(i) * n_tp + s,
        x_recv_sem,
        x_ts,
    )
    x_beside = remote(x_send.at[sibling], x_recv.at[ep], x_own.at[0], x_own.at[1], sibling, t)

    def l_to(d):
        mine = kv_buf.at[ep, t]
        return remote(mine, mine, lat_zs.at[d], lat_recv.at[ep * n_tp + t], plane(d) * 2 + core, t)

    def l_from(i):
        return source(1 + i) * 2 + core

    latents = Spread(
        nz - 1,
        n_tp,
        ep,
        t,
        lambda i, s: kv_buf.at[l_from(i), s],
        lambda i, s: l_from(i) * n_tp + s,
        lat_recv,
        lat_ts,
        (lat_recv, lat_cs),
    )
    l_beside = remote(kv_buf.at[ep], kv_buf.at[ep], lat_own.at[0], lat_own.at[1], sibling, t)

    projection = Spread(
        pieces,
        n_tp,
        ep,
        t,
        lambda i, s: wo.at[s, pl.ds(pl.multiple_of((core * pieces + i) * slab, slab), slab), :],
        lambda i, s: i * n_tp + s,
        wo_recv,
        wo_ts,
        (wo_crecv, wo_cs),
    )

    l_beside.start()
    x_beside.start()
    loop(n_ep - 2, lambda i: x_to(i).start())
    loop(nz, lambda d: l_to(d).start(), 1)
    loads[0].wait()
    projection.push(0)

    def beside(parts, height, filled):
        filler = jnp.zeros((height, LANES - filled), BF)
        return jnp.concatenate(parts + [filler], axis=1)

    for h in range(heads):
        nope, value = slice(h * NOPE, (h + 1) * NOPE), slice(h * VDIM, (h + 1) * VDIM)
        w_ref[:, h * LANES : (h + 1) * LANES] = beside([wk_ref[:, nope]], lat, NOPE)
        w_ref[:, wide + h * LANES : wide + (h + 1) * LANES] = beside([wv_ref[:, value]], lat, VDIM)
    normed = rms_rows(lat_ref[...], gain_ref[:, :deep])
    for h in range(heads):
        turn = qr_ref[:, h * ROPE : (h + 1) * ROPE]
        plain = beside([qn_ref[:, h * NOPE : (h + 1) * NOPE], turn], deep, NOPE + ROPE)
        blank = jnp.zeros((deep, NOPE), BF)
        turned = beside([blank, -turn[:, half:], turn[:, :half]], deep, NOPE + ROPE)
        q = jnp.dot(normed, plain, preferred_element_type=F32) * cos
        q = q + jnp.dot(normed, turned, preferred_element_type=F32) * sin
        q_ref[h] = q.astype(BF)

    keys = 2 * rows
    q_block = min(256, rows)

    def project(d):
        for j in range(2):
            block = kv_buf[source(d) * 2 + j]
            tall = block[:, :part, :].reshape(rows, lat)
            up = jnp.dot(tall, w_ref[...], preferred_element_type=F32)
            pieces_ = []
            for s in range(n_tp):
                packed = block[s, part:, :].astype(F32)
                for g in range(part // BAND):
                    b, q = g // 8, g % 8 // 4
                    piece = packed[b * BAND : (b + 1) * BAND, q * LANES : (q + 1) * LANES]
                    shift = (NOPE - 32 * (g % 4)) % LANES
                    pieces_.append(pltpu.roll(piece, shift, 1) if shift else piece)
            turned = jnp.concatenate(pieces_, axis=0)
            spot = lax.broadcasted_iota(jnp.int32, (rows, LANES), 1)
            turned = jnp.where((spot >= NOPE) & (spot < NOPE + ROPE), turned, 0.0)
            at = slice(j * rows, (j + 1) * rows)
            for h in range(heads):
                k_buf[h, at, :] = (up[:, h * LANES : (h + 1) * LANES] + turned).astype(BF)
                v = up[:, wide + h * LANES : wide + (h + 1) * LANES]
                v_buf[h, at, :] = jnp.where(spot < VDIM, v, 1.0).astype(BF)

    def attend(h, here):
        s = lax.dot_general(
            q_ref[h, here, :], k_buf[h], (((1,), (1,)), ((), ())), preferred_element_type=F32
        )
        old = top_ref[h, here, :1]
        top = jnp.maximum(old, jnp.max(s, axis=-1, keepdims=True))
        p = jnp.exp2((s - top) * scale).astype(BF)
        pv = jnp.dot(p, v_buf[h], preferred_element_type=F32)
        acc_ref[h, here, :] = acc_ref[h, here, :] * jnp.exp2((old - top) * scale) + pv
        top_ref[h, here, :] = jnp.broadcast_to(top, (q_block, LANES))

    together = min(2, heads)
    beats = rows // q_block * heads // together

    def beat(i):
        at = i // (heads // together)
        here = pl.ds(pl.multiple_of(at * q_block, q_block), q_block)
        for h in range(together):
            attend(i % (heads // together) * together + h, here)

    top_ref[...] = jnp.full(top_ref.shape, -jnp.inf, F32)
    acc_ref[...] = jnp.zeros(acc_ref.shape, F32)

    total = n_ep * room
    step = min(256, hid.shape[1])

    def up(i):
        at = pl.ds(pl.multiple_of(i * step, step), step)
        x = x_recv[...].reshape(total, width)
        g = jnp.dot(x, wg[:, at], preferred_element_type=F32)
        u = jnp.dot(x, wu[:, at], preferred_element_type=F32)
        hid[:, at] = (g / (1.0 + jnp.exp(-g)) * u).astype(BF)

    def to_tp(src, recv, ss, rs, d):
        return remote(src, recv.at[t], ss.at[d], rs.at[t], ep, (t + d) % n_tp)

    def from_tp(recv, ss, rs, d):
        frm = (t + n_tp - d) % n_tp
        remote(recv.at[frm], recv.at[frm], ss.at[0], rs.at[frm], ep, frm).wait_recv()
        return frm

    def to_ep(d):
        to = (ep + d) % n_ep
        return remote(e_send.at[to], e_recv.at[ep], es.at[d], er.at[ep], to, t)

    square = n_tp == 4
    part_w = share // 2
    xn, yn, dn = routed.at(1), routed.at(2), routed.at(3 if square else 1)
    plan = [(dn, 0, xn, 0), (dn, 1, yn, 1), (xn, 0, xn, 2), (yn, 1, yn, 3)]
    kept = [(yn, 0, yn, 4), (xn, 1, xn, 5), (t, 0, None, 6), (t, 1, None, 7)]

    def hop(k):
        to = (plan + kept)[k][2]
        return remote(t_send.at[k], t_recv.at[k], ts.at[k], tr.at[k], ep, to)

    def term(d):
        return to_tp(t_send.at[(t + d) % n_tp], t_recv, ts, tr, d)

    def summed_columns(k):
        group, part_at = (plan + kept)[k][:2]
        at = pl.ds(pl.multiple_of(group * share + part_at * part_w, part_w), part_w)
        t_send[k] = jnp.dot(hid[...], wd[:, at], preferred_element_type=F32).astype(BF)

    def down(d):
        to = (t + d) % n_tp
        t_send[to] = jnp.dot(hid[...], wd[:, columns(to)], preferred_element_type=F32).astype(BF)

        @pl.when(d < n_tp)
        def _():
            term(d).start()

    def experts_up():
        loads[1].wait()
        loads[2].wait()
        loop(hid.shape[1] // step, up)
        loads[3].wait()

    def experts_down():
        if square:
            for k in range(8):
                summed_columns(k)
                if k < 4:
                    hop(k).start()
        else:
            loop(n_tp + 1, down, 1)

    def second_hop():
        if square:
            for k in range(2):
                hop(k).wait_recv()
                t_send[4 + k] = (t_send[4 + k].astype(F32) + t_recv[k].astype(F32)).astype(BF)
                hop(4 + k).start()

    def give_back():
        if square:
            for k in range(2):
                hop(2 + k).wait_recv()
                hop(4 + k).wait_recv()
                out = t_send[6 + k].astype(F32) + t_recv[2 + k].astype(F32) + t_recv[4 + k].astype(F32)
                e_send[:, :, k * part_w : (k + 1) * part_w] = out.astype(BF).reshape(n_ep, room, part_w)
        else:
            out = t_send[t].astype(F32)
            for d in range(1, n_tp):
                out = out + t_recv[from_tp(t_recv, ts, tr, d)].astype(F32)
            e_send[...] = out.astype(BF).reshape(n_ep, room, share)
        e_recv[ep] = e_send[ep]
        loop(n_ep, lambda d: to_ep(d).start(), 1)

    def plane_landed(d):
        def beside_landed(s):
            at = source(d) * 2 + 1 - core
            ref = kv_buf.at[at, s]
            remote(ref, ref, lat_own.at[0], lat_recv.at[at * n_tp + s], sibling, t).wait_recv()

        @pl.when(d == 0)
        def _():
            l_beside.wait_recv()

        @pl.when(d > 0)
        def _():
            loop(n_tp, beside_landed)

    def some(count, body, k, of):
        low, high = count * k // of, count * (k + 1) // of
        if high > low:
            loop(high, body, low)

    def lat_push(k, of):
        some(nz - 1, lambda i: (latents.landed(i, 0), latents.push(i), latents.across(i, 0).start()), k, of)

    def x_push(k, of):
        some(n_ep - 2, lambda i: (routed.landed(i, 0), routed.push(i)), k, of)

    def x_relay(k, of):
        some(n_ep - 2, routed.relay, k, of)

    def lat_relay(k, of):
        some(nz - 1, latents.relay, k, of)

    def lat_last(k, of):
        some(nz - 1, latents.last, k, of)

    def wo_relay(k, of):
        some(pieces, projection.relay, k, of)

    def x_last():
        x_beside.wait_recv()
        loop(n_ep - 2, routed.last)

    events = [
        (0, [lambda: x_push(0, 6)]),
        (1, [lambda: x_push(1, 6)]),
        (2, [lambda: x_push(2, 6)]),
        (3, [lambda: x_push(3, 6), lambda: x_relay(0, 6)]),
        (4, [
            lambda: x_push(4, 6),
            lambda: x_relay(1, 6),
            lambda: x_push(5, 6),
            lambda: x_relay(2, 6),
            lambda: x_relay(3, 6),
            lambda: x_relay(4, 6),
            lambda: lat_push(0, 3),
            lambda: x_relay(5, 6),
            lambda: lat_push(1, 3),
            lambda: x_last(),
            lambda: experts_up(),
            lambda: lat_push(2, 3),
            lambda: lat_relay(0, 3),
            lambda: lat_relay(1, 3),
            lambda: experts_down(),
            lambda: lat_relay(2, 3),
            lambda: lat_last(0, 3),
        ]),
        (6, [lambda: lat_last(1, 3)]),
        (8, [
            lambda: second_hop(),
            lambda: loop(pieces, projection.push, 1),
            lambda: wo_relay(0, 4),
            lambda: lat_last(2, 3),
        ]),
        (12, [lambda: wo_relay(1, 4)]),
        (14, [lambda: wo_relay(2, 4), lambda: give_back()]),
        (15, [lambda: wo_relay(3, 4)]),
    ]

    def one(j):
        for at, todo in events:
            @pl.when(j == at * beats // 4)
            def _(todo=todo):
                for call in todo:
                    call()

        @pl.when(j % beats == 0)
        def _():
            plane_landed(j // beats)
            project(j // beats)

        beat(j % beats)

    loop(nz * beats, one)

    def finish(i):
        here = pl.ds(pl.multiple_of(i * q_block, q_block), q_block)
        done = []
        for h in range(heads):
            acc = acc_ref[h, here, :]
            done.append((acc[:, :VDIM] / acc[:, VDIM : VDIM + 1]).astype(BF))
        att_ref[here, :] = done[0] if heads == 1 else jnp.concatenate(done, axis=1)

    loop(rows // q_block, finish)

    def piece_of(s):
        return pl.ds(pl.multiple_of(s * part, part), part)

    def attended(d):
        return to_tp(att_ref.at[piece_of((t + d) % n_tp), :], a_buf, as_, ar, d)

    loop(n_tp, lambda d: attended(d).start(), 1)
    a_buf[t] = att_ref[piece_of(t), :]
    loop(pieces, projection.last)

    def across_landed(i):
        def one(d):
            owner = projection.frm(d)
            at = pl.ds(pl.multiple_of(((1 - core) * pieces + i) * slab, slab), slab)
            ref = wo.at[owner, at, :]
            remote(ref, ref, wo_cs.at[0], wo_crecv.at[i * n_tp + owner], sibling, t).wait_recv()

        loop(n_tp, one, 1)

    loop(pieces, across_landed)
    for d in range(1, n_tp):
        from_tp(a_buf, as_, ar, d)

    def mix(s):
        at = pl.ds(pl.multiple_of(s * span, span), span)
        out = jnp.zeros((part, span), F32)
        for g in range(n_tp):
            out = out + jnp.dot(a_buf[g], wo[g, :, at], preferred_element_type=F32)
        mix_ref[:, at] = out.astype(BF)

    loop(width // span, mix)

    def arrived(d):
        frm = (ep + n_ep - d) % n_ep
        remote(e_recv.at[frm], e_recv.at[frm], es.at[0], er.at[frm], frm, t).wait_recv()

    loop(n_ep, arrived, 1)
    home = e_recv[...].reshape(total, share)
    out = jnp.dot(own_hi[...], home, preferred_element_type=F32)
    out = out + jnp.dot(own_lo[...], home, preferred_element_type=F32)
    exp_ref[...] = out.astype(BF)

    l_beside.wait_send()
    x_beside.wait_send()
    loop(n_ep - 2, lambda i: (x_to(i).wait_send(), routed.drain(i)))
    loop(nz, lambda d: l_to(d).wait_send(), 1)
    loop(nz - 1, lambda i: latents.drain(i, 0))
    loop(pieces, projection.drain)
    if square:
        for k in range(6):
            hop(k).wait_send()
    else:
        loop(n_tp, lambda d: term(d).wait_send(), 1)
    loop(n_tp, lambda d: attended(d).wait_send(), 1)
    loop(n_ep, lambda d: to_ep(d).wait_send(), 1)


def turn_tables(n_ep, rows):
    half = ROPE // 2
    freqs = 10000.0 ** (-np.arange(half) / half)
    lanes = np.zeros(LANES)
    lanes[NOPE : NOPE + half] = freqs
    lanes[NOPE + half : NOPE + ROPE] = freqs
    near = np.arange(rows)[:, None] * lanes
    far = (np.arange(n_ep) * rows)[:, None] * lanes
    return [f(a).astype(np.float32) for a in (near, far) for f in (np.cos, np.sin)]


def mega(n_ep, n_tp, heads, operands, w_out, w_gate, w_up, w_down):
    kv, rope, latent = operands[:3]
    tokens = operands[12]
    rows = latent.shape[0]
    rows_b, width = tokens.shape
    lat = kv.shape[1]
    part = rows // n_tp
    unit = part + -(-part // LANES) * BAND
    room = -(-(3 * rows_b // n_ep) // BAND) * BAND
    total = n_ep * room
    share = width // n_tp
    hidden = w_gate.shape[1]
    nz = n_ep // 2
    depth = w_out.shape[0]
    pieces = min(4, depth // 2 // BAND)
    vmem = pl.BlockSpec(memory_space=pltpu.VMEM)
    hbm = pl.BlockSpec(memory_space=pl.ANY)
    dma = pltpu.SemaphoreType.DMA
    keys = rows * n_ep
    flops = 4 * heads * rows * keys * 256 + 6 * total * width * hidden
    return pl.pallas_call(
        functools.partial(mega_kernel, heads, n_ep, n_tp),
        out_shape=(
            jax.ShapeDtypeStruct((part, width), BF),
            jax.ShapeDtypeStruct((rows_b, share), BF),
        ),
        in_specs=[vmem] * len(operands) + [hbm] * 4,
        out_specs=(vmem, vmem),
        scratch_shapes=[
            pltpu.VMEM((n_tp,) + w_out.shape, BF),
            pltpu.VMEM(w_gate.shape, BF),
            pltpu.VMEM(w_up.shape, BF),
            pltpu.VMEM(w_down.shape, BF),
            pltpu.VMEM((n_ep, n_tp, unit, lat), BF),
            pltpu.VMEM((heads, 2 * rows, LANES), BF),
            pltpu.VMEM((heads, 2 * rows, LANES), BF),
            pltpu.VMEM((heads, rows, LANES), BF),
            pltpu.VMEM((lat, 2 * heads * LANES), BF),
            pltpu.VMEM((heads, rows, LANES), F32),
            pltpu.VMEM((heads, rows, LANES), F32),
            pltpu.VMEM((rows, heads * VDIM), BF),
            pltpu.VMEM((n_tp, part, heads * VDIM), BF),
            pltpu.VMEM((n_ep, room, width), BF),
            pltpu.VMEM((n_ep, room, width), BF),
            pltpu.VMEM((total, hidden), BF),
            pltpu.VMEM((8, total, share // 2) if n_tp == 4 else (n_tp, total, share), BF),
            pltpu.VMEM((6, total, share // 2) if n_tp == 4 else (n_tp, total, share), BF),
            pltpu.VMEM((n_ep, room, share), BF),
            pltpu.VMEM((n_ep, room, share), BF),
            pltpu.VMEM((rows_b, total), BF),
            pltpu.VMEM((rows_b, total), BF),
            dma((4,)),
            dma((nz,)),
            dma((nz * n_tp,)),
            dma((nz * n_tp,)),
            dma((n_ep * n_tp,)),
            dma((2,)),
            dma((n_ep,)),
            dma((n_ep * n_tp,)),
            dma((n_ep * n_tp,)),
            dma((2,)),
            dma((pieces * n_tp,)),
            dma((pieces * n_tp,)),
            dma((pieces * n_tp,)),
            dma((pieces * n_tp,)),
            dma((n_tp,)),
            dma((n_tp,)),
            dma((max(6, n_tp),)),
            dma((max(6, n_tp),)),
            dma((n_ep,)),
            dma((n_ep,)),
        ],
        compiler_params=pltpu.CompilerParams(
            vmem_limit_bytes=60 * 1024 * 1024, collective_id=0, has_side_effects=True
        ),
        cost_estimate=pl.CostEstimate(
            flops=flops, bytes_accessed=20 * 1024 * 1024, transcendentals=heads * rows * keys
        ),
        name="mega",
    )(*operands, w_out, w_gate, w_up, w_down)


def shards(
    q_latent,
    kv_latent,
    rope_key,
    q_gain,
    kv_gain,
    w_q_nope,
    w_q_rope,
    w_k_nope,
    w_value,
    w_out,
    tokens_b,
    norm_gain_b,
    routes,
    route_logits,
    w_gate,
    w_up,
    w_down,
):
    n_ep = lax.axis_size("ep")
    n_tp = lax.axis_size("tp")
    heads = w_q_nope.shape[1] // NOPE
    cos_b, sin_b, cos_a, sin_a = turn_tables(n_ep, q_latent.shape[0])
    operands = (
        kv_latent,
        rope_key.T,
        q_latent,
        jnp.concatenate([q_gain, kv_gain, norm_gain_b])[None, :],
        cos_b,
        sin_b,
        cos_a,
        sin_a,
        w_q_nope,
        w_q_rope,
        w_k_nope,
        w_value,
        tokens_b,
        routes.T,
        route_logits.T,
    )
    return mega(n_ep, n_tp, heads, operands, w_out, w_gate[0], w_up[0], w_down[0])


def solution(mesh):
    placed = (
        P("ep", None),
        P("ep", None),
        P("ep", None),
        P(),
        P(),
        P(None, "tp"),
        P(None, "tp"),
        P(None, "tp"),
        P(None, "tp"),
        P("tp", None),
        P("ep", None),
        P(),
        P("ep", None),
        P("ep", None),
        P("ep", None, "tp"),
        P("ep", None, "tp"),
        P("ep", "tp", None),
    )
    return jax.shard_map(
        shards,
        mesh=mesh,
        in_specs=placed,
        out_specs=(P(("ep", "tp"), None), P("ep", "tp")),
        check_vma=False,
    )
```

```python
import functools
import math

import jax
import jax.numpy as jnp
import numpy as np
from jax import lax
from jax.experimental import pallas as pl
from jax.experimental.pallas import tpu as pltpu
from jax.sharding import PartitionSpec as P

NOPE = 64
ROPE = 32
VDIM = 64
LANES = 128
BAND = 16
EPSILON = 1e-06
BF = jnp.bfloat16
F32 = jnp.float32
MESH = pl.DeviceIdType.MESH


def rms_rows(values, gain):
    wide = values.astype(F32)
    scaled = wide * lax.rsqrt(jnp.mean(wide * wide, axis=-1, keepdims=True) + EPSILON)
    return (scaled * gain.astype(F32)).astype(BF)


def remote(src, dst, send, recv, ep, tp):
    return pltpu.make_async_remote_copy(
        src_ref=src,
        dst_ref=dst,
        send_sem=send,
        recv_sem=recv,
        device_id={"ep": ep, "tp": tp},
        device_id_type=MESH,
    )


def loop(count, body, start=0):
    def step(i, c):
        body(i)
        return c

    lax.fori_loop(start, count, step, 0)


class Spread:
    def __init__(self, count, n_tp, ep, t, view, index, recv, send, sib=None):
        self.count, self.n_tp, self.ep, self.t = count, n_tp, ep, t
        self.view, self.index, self.recv, self.send = view, index, recv, send
        self.square = n_tp == 4
        self.direct = 3 if self.square else n_tp
        self.sib = sib

    def at(self, d):
        if self.square:
            return (self.t // 2 + d // 2) % 2 * 2 + (self.t % 2 + d % 2) % 2
        return (self.t + d) % self.n_tp

    def frm(self, d):
        return self.at(d) if self.square else (self.t + self.n_tp - d) % self.n_tp

    def copy(self, i, d):
        ref = self.view(i, self.t)
        sem = self.recv.at[self.index(i, self.t)]
        return remote(ref, ref, self.send.at[i * self.n_tp + d], sem, self.ep, self.at(d))

    def passed(self, i):
        owner = self.at(1 + i % 2)
        ref = self.view(i, owner)
        sem = self.recv.at[self.index(i, owner)]
        return remote(ref, ref, self.send.at[i * self.n_tp + 3], sem, self.ep, self.at(2 - i % 2))

    def across(self, i, d):
        owner = self.frm(d)
        ref = self.view(i, owner)
        recv, send = self.sib
        sem = recv.at[self.index(i, owner)]
        return remote(ref, ref, send.at[i * self.n_tp + d], sem, self.ep // 2 * 2 + 1 - self.ep % 2, self.t)

    def landed(self, i, d):
        owner = self.frm(d)
        ref = self.view(i, owner)
        remote(ref, ref, self.send.at[0], self.recv.at[self.index(i, owner)], self.ep, self.t).wait_recv()

    def push(self, i):
        loop(self.direct, lambda d: self.copy(i, d).start(), 1)

    def relay(self, i):
        def one(d):
            self.landed(i, d)
            if self.sib is not None:
                self.across(i, d).start()

        loop(self.direct, one, 1)
        if self.square:
            self.passed(i).start()

    def last(self, i):
        if self.square:
            self.landed(i, 3)
            if self.sib is not None:
                self.across(i, 3).start()

    def drain(self, i, first=1):
        loop(self.direct, lambda d: self.copy(i, d).wait_send(), 1)
        if self.square:
            self.passed(i).wait_send()
        if self.sib is not None:
            loop(self.n_tp, lambda d: self.across(i, d).wait_send(), first)


def mega_kernel(
    heads,
    n_ep,
    n_tp,
    kv_ref,
    rope_ref,
    lat_ref,
    gain_ref,
    cosb_ref,
    sinb_ref,
    cosa_ref,
    sina_ref,
    qn_ref,
    qr_ref,
    wk_ref,
    wv_ref,
    tokb_ref,
    route_ref,
    logit_ref,
    wo_hbm,
    wg_hbm,
    wu_hbm,
    wd_hbm,
    mix_ref,
    exp_ref,
    wo,
    wg,
    wu,
    wd,
    kv_buf,
    k_buf,
    v_buf,
    q_ref,
    w_ref,
    acc_ref,
    top_ref,
    att_ref,
    a_buf,
    x_send,
    x_recv,
    hid,
    t_send,
    t_recv,
    e_send,
    e_recv,
    own_hi,
    own_lo,
    w_sem,
    lat_zs,
    lat_ts,
    lat_cs,
    lat_recv,
    lat_own,
    x_zs,
    x_ts,
    x_recv_sem,
    x_own,
    wo_ts,
    wo_recv,
    wo_cs,
    wo_crecv,
    as_,
    ar,
    ts,
    tr,
    es,
    er,
):
    ep, t = lax.axis_index("ep"), lax.axis_index("tp")
    nz = n_ep // 2
    z, core = ep // 2, ep % 2
    sibling = z * 2 + 1 - core
    rows, deep = lat_ref.shape
    lat = wk_ref.shape[0]
    unit = kv_buf.shape[2]
    part = rows // n_tp
    room, width = x_send.shape[1:]
    share = width // n_tp
    rows_b = tokb_ref.shape[0]
    depth = wo.shape[1]
    pieces = wo_ts.shape[0] // n_tp
    slab = depth // 2 // pieces
    half = ROPE // 2
    scale = (NOPE + ROPE) ** (-0.5) * math.log2(math.e)
    wide = heads * LANES

    loads = [
        pltpu.make_async_copy(a, b, w_sem.at[i])
        for i, (a, b) in enumerate(((wo_hbm, wo.at[t]), (wg_hbm, wg), (wu_hbm, wu), (wd_hbm, wd)))
    ]
    for load in loads:
        load.start()

    barrier = pltpu.get_barrier_semaphore()

    def hello(e, tp):
        pl.semaphore_signal(barrier, inc=1, device_id={"ep": e, "tp": tp}, device_id_type=MESH)

    loop(n_tp, lambda d: hello(ep, (t + d) % n_tp), 1)
    loop(n_ep, lambda d: hello((ep + d) % n_ep, t), 1)

    def columns(s):
        return pl.ds(pl.multiple_of(s * share, share), share)

    def plane(d):
        return (z + d) % nz

    def source(d):
        return (z + nz - d) % nz

    slots = n_ep * room
    lane = lax.broadcasted_iota(jnp.int32, (rows_b, slots), 1)
    expert = jnp.floor((lane.astype(F32) + 0.5) * (1.0 / room))
    place = lane.astype(F32) - expert * room
    def standing(ref):
        return jnp.transpose(jnp.broadcast_to(ref[:1, :], (8, rows_b))), jnp.transpose(
            jnp.broadcast_to(ref[1:2, :], (8, rows_b))
        )

    route = [x[:, :1] for x in standing(route_ref[...].astype(F32))]
    first, second = route[0] == expert, route[1] == expert
    named = (first | second).astype(F32)
    r = lax.broadcasted_iota(jnp.int32, (rows_b, rows_b), 0)
    c = lax.broadcasted_iota(jnp.int32, (rows_b, rows_b), 1)
    ahead = jnp.dot((c < r).astype(F32).astype(BF), named.astype(BF), preferred_element_type=F32)
    mine = jnp.where(ahead == place, named, 0.0)
    logits = logit_ref[...]
    peak = jnp.max(logits, axis=0, keepdims=True)
    grown = jnp.exp(logits - peak)
    weights = [x[:, :1] for x in standing(grown / jnp.sum(grown, axis=0, keepdims=True))]
    weighted = mine * jnp.where(first, weights[0], weights[1])
    high = weighted.astype(BF)
    own_hi[...] = high
    own_lo[...] = (weighted - high.astype(F32)).astype(BF)

    normed_b = rms_rows(tokb_ref[...], gain_ref[:, deep + lat :])
    pick = jnp.transpose(mine).astype(BF)
    span = min(512, width)
    for s in range(width // span):
        got = jnp.dot(pick, normed_b[:, s * span : (s + 1) * span], preferred_element_type=F32)
        x_send[:, :, s * span : (s + 1) * span] = got.astype(BF).reshape(n_ep, room, span)
    x_recv[ep] = x_send[ep]

    cos_a, sin_a = cosa_ref[pl.ds(ep, 1), :], sina_ref[pl.ds(ep, 1), :]
    cos = cos_a * cosb_ref[...] - sin_a * sinb_ref[...]
    sin = sin_a * cosb_ref[...] + cos_a * sinb_ref[...]
    normed_kv = rms_rows(kv_ref[...], gain_ref[:, deep : deep + lat])
    raw = jnp.transpose(rope_ref[...].astype(F32))
    front = jnp.zeros((rows, NOPE), F32)
    back = jnp.zeros((rows, LANES - NOPE - ROPE), F32)
    plain = jnp.concatenate([front, raw, back], axis=1)
    turned = jnp.concatenate([front, -raw[:, half:], raw[:, :half], back], axis=1)
    rot = plain * cos + turned * sin
    for s in range(n_tp):
        kv_buf[ep, s, :part, :] = normed_kv[s * part : (s + 1) * part]
        bands = [jnp.zeros((BAND, LANES), F32)] * ((unit - part) // BAND * 2)
        for g in range(part // BAND):
            at = s * part + g * BAND
            shift = (32 * (g % 4) - NOPE) % LANES
            piece = rot[at : at + BAND]
            bands[g // 4] = bands[g // 4] + (pltpu.roll(piece, shift, 1) if shift else piece)
        for b in range(len(bands) // 2):
            pair = jnp.concatenate(bands[2 * b : 2 * b + 2], axis=1).astype(BF)
            kv_buf[ep, s, part + b * BAND : part + (b + 1) * BAND, :] = pair

    pl.semaphore_wait(barrier, n_tp + n_ep - 2)

    def x_to(i):
        to = plane(1 + i // 2) * 2 + i % 2
        at = columns(t)
        return remote(
            x_send.at[to, :, at],
            x_recv.at[ep, :, at],
            x_zs.at[i],
            x_recv_sem.at[ep * n_tp + t],
            to,
            t,
        )

    def x_from(i):
        return source(1 + i // 2) * 2 + i % 2

    routed = Spread(
        n_ep - 2,
        n_tp,
        ep,
        t,
        lambda i, s: x_recv.at[x_from(i), :, columns(s)],
        lambda i, s: x_from(i) * n_tp + s,
        x_recv_sem,
        x_ts,
    )
    x_beside = remote(x_send.at[sibling], x_recv.at[ep], x_own.at[0], x_own.at[1], sibling, t)

    def l_to(d):
        mine = kv_buf.at[ep, t]
        return remote(mine, mine, lat_zs.at[d], lat_recv.at[ep * n_tp + t], plane(d) * 2 + core, t)

    def l_from(i):
        return source(1 + i) * 2 + core

    latents = Spread(
        nz - 1,
        n_tp,
        ep,
        t,
        lambda i, s: kv_buf.at[l_from(i), s],
        lambda i, s: l_from(i) * n_tp + s,
        lat_recv,
        lat_ts,
        (lat_recv, lat_cs),
    )
    l_beside = remote(kv_buf.at[ep], kv_buf.at[ep], lat_own.at[0], lat_own.at[1], sibling, t)

    projection = Spread(
        pieces,
        n_tp,
        ep,
        t,
        lambda i, s: wo.at[s, pl.ds(pl.multiple_of((core * pieces + i) * slab, slab), slab), :],
        lambda i, s: i * n_tp + s,
        wo_recv,
        wo_ts,
        (wo_crecv, wo_cs),
    )

    l_beside.start()
    x_beside.start()
    loop(n_ep - 2, lambda i: x_to(i).start())
    loads[0].wait()
    loop(pieces // 4, projection.push)

    def beside(parts, height, filled):
        filler = jnp.zeros((height, LANES - filled), BF)
        return jnp.concatenate(parts + [filler], axis=1)

    for h in range(heads):
        nope, value = slice(h * NOPE, (h + 1) * NOPE), slice(h * VDIM, (h + 1) * VDIM)
        w_ref[:, h * LANES : (h + 1) * LANES] = beside([wk_ref[:, nope]], lat, NOPE)
        w_ref[:, wide + h * LANES : wide + (h + 1) * LANES] = beside([wv_ref[:, value]], lat, VDIM)
    normed = rms_rows(lat_ref[...], gain_ref[:, :deep])
    for h in range(heads):
        turn = qr_ref[:, h * ROPE : (h + 1) * ROPE]
        plain = beside([qn_ref[:, h * NOPE : (h + 1) * NOPE], turn], deep, NOPE + ROPE)
        blank = jnp.zeros((deep, NOPE), BF)
        turned = beside([blank, -turn[:, half:], turn[:, :half]], deep, NOPE + ROPE)
        q = jnp.dot(normed, plain, preferred_element_type=F32) * cos
        q = q + jnp.dot(normed, turned, preferred_element_type=F32) * sin
        q_ref[h] = q.astype(BF)

    keys = 2 * rows
    q_block = min(256, rows)

    def project(d):
        for j in range(2):
            block = kv_buf[source(d) * 2 + j]
            tall = block[:, :part, :].reshape(rows, lat)
            up = jnp.dot(tall, w_ref[...], preferred_element_type=F32)
            pieces_ = []
            for s in range(n_tp):
                packed = block[s, part:, :].astype(F32)
                for g in range(part // BAND):
                    b, q = g // 8, g % 8 // 4
                    piece = packed[b * BAND : (b + 1) * BAND, q * LANES : (q + 1) * LANES]
                    shift = (NOPE - 32 * (g % 4)) % LANES
                    pieces_.append(pltpu.roll(piece, shift, 1) if shift else piece)
            turned = jnp.concatenate(pieces_, axis=0)
            spot = lax.broadcasted_iota(jnp.int32, (rows, LANES), 1)
            turned = jnp.where((spot >= NOPE) & (spot < NOPE + ROPE), turned, 0.0)
            at = slice(j * rows, (j + 1) * rows)
            for h in range(heads):
                k_buf[h, at, :] = (up[:, h * LANES : (h + 1) * LANES] + turned).astype(BF)
                v = up[:, wide + h * LANES : wide + (h + 1) * LANES]
                v_buf[h, at, :] = jnp.where(spot < VDIM, v, 1.0).astype(BF)

    def attend(h, here):
        s = lax.dot_general(
            q_ref[h, here, :], k_buf[h], (((1,), (1,)), ((), ())), preferred_element_type=F32
        )
        old = top_ref[h, here, :1]
        top = jnp.maximum(old, jnp.max(s, axis=-1, keepdims=True))
        p = jnp.exp2((s - top) * scale).astype(BF)
        pv = jnp.dot(p, v_buf[h], preferred_element_type=F32)
        acc_ref[h, here, :] = acc_ref[h, here, :] * jnp.exp2((old - top) * scale) + pv
        top_ref[h, here, :] = jnp.broadcast_to(top, (q_block, LANES))

    together = min(2, heads)
    beats = rows // q_block * heads // together

    def beat(i):
        at = i // (heads // together)
        here = pl.ds(pl.multiple_of(at * q_block, q_block), q_block)
        for h in range(together):
            attend(i % (heads // together) * together + h, here)

    top_ref[...] = jnp.full(top_ref.shape, -jnp.inf, F32)
    acc_ref[...] = jnp.zeros(acc_ref.shape, F32)

    total = n_ep * room
    step = min(256, hid.shape[1])

    def up(i):
        at = pl.ds(pl.multiple_of(i * step, step), step)
        x = x_recv[...].reshape(total, width)
        g = jnp.dot(x, wg[:, at], preferred_element_type=F32)
        u = jnp.dot(x, wu[:, at], preferred_element_type=F32)
        hid[:, at] = (g / (1.0 + jnp.exp(-g)) * u).astype(BF)

    def to_tp(src, recv, ss, rs, d):
        return remote(src, recv.at[t], ss.at[d], rs.at[t], ep, (t + d) % n_tp)

    def from_tp(recv, ss, rs, d):
        frm = (t + n_tp - d) % n_tp
        remote(recv.at[frm], recv.at[frm], ss.at[0], rs.at[frm], ep, frm).wait_recv()
        return frm

    def to_ep(d):
        to = (ep + d) % n_ep
        return remote(e_send.at[to], e_recv.at[ep], es.at[d], er.at[ep], to, t)

    square = n_tp == 4
    part_w = share // 2
    xn, yn, dn = routed.at(1), routed.at(2), routed.at(3 if square else 1)
    plan = [(dn, 0, xn, 0), (dn, 1, yn, 1), (xn, 0, xn, 2), (yn, 1, yn, 3)]
    kept = [(yn, 0, yn, 4), (xn, 1, xn, 5), (t, 0, None, 6), (t, 1, None, 7)]

    def hop(k):
        to = (plan + kept)[k][2]
        return remote(t_send.at[k], t_recv.at[k], ts.at[k], tr.at[k], ep, to)

    def term(d):
        return to_tp(t_send.at[(t + d) % n_tp], t_recv, ts, tr, d)

    def summed_columns(k):
        group, part_at = (plan + kept)[k][:2]
        at = pl.ds(pl.multiple_of(group * share + part_at * part_w, part_w), part_w)
        t_send[k] = jnp.dot(hid[...], wd[:, at], preferred_element_type=F32).astype(BF)

    def down(d):
        to = (t + d) % n_tp
        t_send[to] = jnp.dot(hid[...], wd[:, columns(to)], preferred_element_type=F32).astype(BF)

        @pl.when(d < n_tp)
        def _():
            term(d).start()

    def experts_up(k, of):
        if k == 0:
            for load in loads[1:]:
                load.wait()
        some(hid.shape[1] // step, up, k, of)

    def experts_down():
        if square:
            for k in range(8):
                summed_columns(k)
                if k < 4:
                    hop(k).start()
        else:
            loop(n_tp + 1, down, 1)

    def second_hop():
        if square:
            for k in range(2):
                hop(k).wait_recv()
                t_send[4 + k] = (t_send[4 + k].astype(F32) + t_recv[k].astype(F32)).astype(BF)
                hop(4 + k).start()

    def give_back():
        if square:
            for k in range(2):
                hop(2 + k).wait_recv()
                hop(4 + k).wait_recv()
                out = t_send[6 + k].astype(F32) + t_recv[2 + k].astype(F32) + t_recv[4 + k].astype(F32)
                e_send[:, :, k * part_w : (k + 1) * part_w] = out.astype(BF).reshape(n_ep, room, part_w)
        else:
            out = t_send[t].astype(F32)
            for d in range(1, n_tp):
                out = out + t_recv[from_tp(t_recv, ts, tr, d)].astype(F32)
            e_send[...] = out.astype(BF).reshape(n_ep, room, share)
        e_recv[ep] = e_send[ep]
        loop(n_ep, lambda d: to_ep(d).start(), 1)

    def plane_landed(d):
        def beside_landed(s):
            at = source(d) * 2 + 1 - core
            ref = kv_buf.at[at, s]
            remote(ref, ref, lat_own.at[0], lat_recv.at[at * n_tp + s], sibling, t).wait_recv()

        @pl.when(d == 0)
        def _():
            l_beside.wait_recv()

        @pl.when(d > 0)
        def _():
            loop(n_tp, beside_landed)

    def some(count, body, k, of):
        low, high = count * k // of, count * (k + 1) // of
        if high > low:
            loop(high, body, low)

    def lat_push(k, of):
        some(nz - 1, lambda i: (latents.landed(i, 0), latents.push(i), latents.across(i, 0).start()), k, of)

    def x_push(k, of):
        some(n_ep - 2, lambda i: (routed.landed(i, 0), routed.push(i)), k, of)

    def x_relay(k, of):
        some(n_ep - 2, routed.relay, k, of)

    def lat_relay(k, of):
        some(nz - 1, latents.relay, k, of)

    def lat_last(k, of):
        some(nz - 1, latents.last, k, of)

    def wo_relay(k, of):
        some(pieces, projection.relay, k, of)

    def x_last():
        x_beside.wait_recv()
        loop(n_ep - 2, routed.last)

    def wo_push(k, of):
        some(pieces, projection.push, k, of)

    def wo_last(k, of):
        some(pieces, projection.last, k, of)

    events = [
        (0, [lambda: x_push(0, 6)]),
        (1, [lambda: x_push(1, 6)]),
        (2, [lambda: x_push(2, 6), lambda: loop(nz, lambda d: l_to(d).start(), 1)]),
        (3, [lambda: x_push(3, 6), lambda: x_relay(0, 6), lambda: x_relay(1, 6)]),
        (4, [
            lambda: x_push(4, 6),
            lambda: x_push(5, 6),
            lambda: x_relay(2, 6),
            lambda: x_relay(3, 6),
            lambda: x_relay(4, 6),
            lambda: x_relay(5, 6),
            lambda: lat_push(0, 3),
            lambda: lat_push(1, 3),
            lambda: x_last(),
            lambda: experts_up(0, 2),
            lambda: lat_push(2, 3),
            lambda: lat_relay(0, 3),
            lambda: lat_relay(1, 3),
            lambda: experts_up(1, 2),
            lambda: lat_relay(2, 3),
            lambda: lat_last(0, 3),
            lambda: experts_down(),
        ]),
        (6, [lambda: second_hop(), lambda: lat_last(1, 3), lambda: loop(pieces, projection.push, 1), lambda: wo_relay(0, 4)]),
        (9, [lambda: lat_last(2, 3)]),
        (11, [lambda: give_back(), lambda: wo_relay(1, 4)]),
        (13, [lambda: wo_relay(2, 4)]),
        (14, [lambda: wo_relay(3, 4), lambda: wo_last(0, 4)]),
        (15, [lambda: wo_last(1, 4)]),
    ]

    def one(j):
        for at, todo in events:
            @pl.when(j == at * beats // 4)
            def _(todo=todo):
                for call in todo:
                    call()

        @pl.when(j % beats == 0)
        def _():
            plane_landed(j // beats)
            project(j // beats)

        beat(j % beats)

    loop(nz * beats, one)

    def finish(i):
        here = pl.ds(pl.multiple_of(i * q_block, q_block), q_block)
        done = []
        for h in range(heads):
            acc = acc_ref[h, here, :]
            done.append((acc[:, :VDIM] / acc[:, VDIM : VDIM + 1]).astype(BF))
        att_ref[here, :] = done[0] if heads == 1 else jnp.concatenate(done, axis=1)

    loop(rows // q_block, finish)

    def piece_of(s):
        return pl.ds(pl.multiple_of(s * part, part), part)

    def attended(d):
        return to_tp(att_ref.at[piece_of((t + d) % n_tp), :], a_buf, as_, ar, d)

    loop(n_tp, lambda d: attended(d).start(), 1)
    a_buf[t] = att_ref[piece_of(t), :]
    wo_last(2, 4)
    wo_last(3, 4)

    def across_landed(i):
        def one(d):
            owner = projection.frm(d)
            at = pl.ds(pl.multiple_of(((1 - core) * pieces + i) * slab, slab), slab)
            ref = wo.at[owner, at, :]
            remote(ref, ref, wo_cs.at[0], wo_crecv.at[i * n_tp + owner], sibling, t).wait_recv()

        loop(n_tp, one, 1)

    loop(pieces, across_landed)
    for d in range(1, n_tp):
        from_tp(a_buf, as_, ar, d)

    def mix(s):
        at = pl.ds(pl.multiple_of(s * span, span), span)
        out = jnp.zeros((part, span), F32)
        for g in range(n_tp):
            out = out + jnp.dot(a_buf[g], wo[g, :, at], preferred_element_type=F32)
        mix_ref[:, at] = out.astype(BF)

    loop(width // span, mix)

    def arrived(d):
        frm = (ep + n_ep - d) % n_ep
        remote(e_recv.at[frm], e_recv.at[frm], es.at[0], er.at[frm], frm, t).wait_recv()

    loop(n_ep, arrived, 1)
    home = e_recv[...].reshape(total, share)
    out = jnp.dot(own_hi[...], home, preferred_element_type=F32)
    out = out + jnp.dot(own_lo[...], home, preferred_element_type=F32)
    exp_ref[...] = out.astype(BF)

    l_beside.wait_send()
    x_beside.wait_send()
    loop(n_ep - 2, lambda i: (x_to(i).wait_send(), routed.drain(i)))
    loop(nz, lambda d: l_to(d).wait_send(), 1)
    loop(nz - 1, lambda i: latents.drain(i, 0))
    loop(pieces, projection.drain)
    if square:
        for k in range(6):
            hop(k).wait_send()
    else:
        loop(n_tp, lambda d: term(d).wait_send(), 1)
    loop(n_tp, lambda d: attended(d).wait_send(), 1)
    loop(n_ep, lambda d: to_ep(d).wait_send(), 1)


def turn_tables(n_ep, rows):
    half = ROPE // 2
    freqs = 10000.0 ** (-np.arange(half) / half)
    lanes = np.zeros(LANES)
    lanes[NOPE : NOPE + half] = freqs
    lanes[NOPE + half : NOPE + ROPE] = freqs
    near = np.arange(rows)[:, None] * lanes
    far = (np.arange(n_ep) * rows)[:, None] * lanes
    return [f(a).astype(np.float32) for a in (near, far) for f in (np.cos, np.sin)]


def mega(n_ep, n_tp, heads, operands, w_out, w_gate, w_up, w_down):
    kv, rope, latent = operands[:3]
    tokens = operands[12]
    rows = latent.shape[0]
    rows_b, width = tokens.shape
    lat = kv.shape[1]
    part = rows // n_tp
    unit = part + -(-part // LANES) * BAND
    room = -(-(3 * rows_b // n_ep) // BAND) * BAND
    total = n_ep * room
    share = width // n_tp
    hidden = w_gate.shape[1]
    nz = n_ep // 2
    depth = w_out.shape[0]
    pieces = min(4, depth // 2 // BAND)
    vmem = pl.BlockSpec(memory_space=pltpu.VMEM)
    hbm = pl.BlockSpec(memory_space=pl.ANY)
    dma = pltpu.SemaphoreType.DMA
    keys = rows * n_ep
    flops = 4 * heads * rows * keys * 256 + 6 * total * width * hidden
    return pl.pallas_call(
        functools.partial(mega_kernel, heads, n_ep, n_tp),
        out_shape=(
            jax.ShapeDtypeStruct((part, width), BF),
            jax.ShapeDtypeStruct((rows_b, share), BF),
        ),
        in_specs=[vmem] * len(operands) + [hbm] * 4,
        out_specs=(vmem, vmem),
        scratch_shapes=[
            pltpu.VMEM((n_tp,) + w_out.shape, BF),
            pltpu.VMEM(w_gate.shape, BF),
            pltpu.VMEM(w_up.shape, BF),
            pltpu.VMEM(w_down.shape, BF),
            pltpu.VMEM((n_ep, n_tp, unit, lat), BF),
            pltpu.VMEM((heads, 2 * rows, LANES), BF),
            pltpu.VMEM((heads, 2 * rows, LANES), BF),
            pltpu.VMEM((heads, rows, LANES), BF),
            pltpu.VMEM((lat, 2 * heads * LANES), BF),
            pltpu.VMEM((heads, rows, LANES), F32),
            pltpu.VMEM((heads, rows, LANES), F32),
            pltpu.VMEM((rows, heads * VDIM), BF),
            pltpu.VMEM((n_tp, part, heads * VDIM), BF),
            pltpu.VMEM((n_ep, room, width), BF),
            pltpu.VMEM((n_ep, room, width), BF),
            pltpu.VMEM((total, hidden), BF),
            pltpu.VMEM((8, total, share // 2) if n_tp == 4 else (n_tp, total, share), BF),
            pltpu.VMEM((6, total, share // 2) if n_tp == 4 else (n_tp, total, share), BF),
            pltpu.VMEM((n_ep, room, share), BF),
            pltpu.VMEM((n_ep, room, share), BF),
            pltpu.VMEM((rows_b, total), BF),
            pltpu.VMEM((rows_b, total), BF),
            dma((4,)),
            dma((nz,)),
            dma((nz * n_tp,)),
            dma((nz * n_tp,)),
            dma((n_ep * n_tp,)),
            dma((2,)),
            dma((n_ep,)),
            dma((n_ep * n_tp,)),
            dma((n_ep * n_tp,)),
            dma((2,)),
            dma((pieces * n_tp,)),
            dma((pieces * n_tp,)),
            dma((pieces * n_tp,)),
            dma((pieces * n_tp,)),
            dma((n_tp,)),
            dma((n_tp,)),
            dma((max(6, n_tp),)),
            dma((max(6, n_tp),)),
            dma((n_ep,)),
            dma((n_ep,)),
        ],
        compiler_params=pltpu.CompilerParams(
            vmem_limit_bytes=60 * 1024 * 1024, collective_id=0, has_side_effects=True
        ),
        cost_estimate=pl.CostEstimate(
            flops=flops, bytes_accessed=20 * 1024 * 1024, transcendentals=heads * rows * keys
        ),
        name="mega",
    )(*operands, w_out, w_gate, w_up, w_down)


def shards(
    q_latent,
    kv_latent,
    rope_key,
    q_gain,
    kv_gain,
    w_q_nope,
    w_q_rope,
    w_k_nope,
    w_value,
    w_out,
    tokens_b,
    norm_gain_b,
    routes,
    route_logits,
    w_gate,
    w_up,
    w_down,
):
    n_ep = lax.axis_size("ep")
    n_tp = lax.axis_size("tp")
    heads = w_q_nope.shape[1] // NOPE
    cos_b, sin_b, cos_a, sin_a = turn_tables(n_ep, q_latent.shape[0])
    operands = (
        kv_latent,
        rope_key.T,
        q_latent,
        jnp.concatenate([q_gain, kv_gain, norm_gain_b])[None, :],
        cos_b,
        sin_b,
        cos_a,
        sin_a,
        w_q_nope,
        w_q_rope,
        w_k_nope,
        w_value,
        tokens_b,
        routes.T,
        route_logits.T,
    )
    return mega(n_ep, n_tp, heads, operands, w_out, w_gate[0], w_up[0], w_down[0])


def solution(mesh):
    placed = (
        P("ep", None),
        P("ep", None),
        P("ep", None),
        P(),
        P(),
        P(None, "tp"),
        P(None, "tp"),
        P(None, "tp"),
        P(None, "tp"),
        P("tp", None),
        P("ep", None),
        P(),
        P("ep", None),
        P("ep", None),
        P("ep", None, "tp"),
        P("ep", None, "tp"),
        P("ep", "tp", None),
    )
    return jax.shard_map(
        shards,
        mesh=mesh,
        in_specs=placed,
        out_specs=(P(("ep", "tp"), None), P("ep", "tp")),
        check_vma=False,
    )
```
